512 devices in a mesh: grp: 2 (over y), ep: 32 (over z, core), tp: 8 (over x).
Axes of the slice: x: 8, y: 2, z: 16, core: 2. Of those that a mesh axis runs over, the one named last changes fastest.
The devices are a block of a 8x8x16 slice.
Arguments:
- tokens: bfloat16 [640, 1024], P(('grp', 'ep')), parts along dimension 0, may hold values from -40 to 40
- attn_gain: float32 [1024], replicated, may hold values from 0.1 to 1.9
- w_query: bfloat16 [1024, 1024], P(None, 'tp'), may hold values from -0.1875 to 0.1875
- w_key: bfloat16 [1024, 512], P(None, 'tp'), may hold values from -0.1875 to 0.1875
- w_value: bfloat16 [1024, 512], P(None, 'tp'), may hold values from -0.1875 to 0.1875
- key_cache: bfloat16 [640, 512, 1024], P(('grp', 'ep'), 'tp'), parts along dimension 0, may hold values from -6 to 6
- value_cache: bfloat16 [640, 512, 1024], P(('grp', 'ep'), 'tp'), parts along dimension 0, may hold values from -6 to 6
- lengths: int32 [640], P(('grp', 'ep')), parts along dimension 0, may hold values from 256 to 1024
- head_bias: float32 [16], P('tp'), may hold values from -8 to -2
- w_out: bfloat16 [1024, 1024], P(None, 'tp'), may hold values from -0.1875 to 0.1875
- ffn_gain: float32 [1024], replicated, may hold values from 0.1 to 1.9
- route_ids: int32 [640, 2], P(('grp', 'ep')), parts along dimension 0, may hold values from 0 to 31, all different within a row; in each aligned block of 10 rows (0 to 9, 10 to 19, ...) at most 2 rows name the same one
- route_weights: float32 [640, 2], P(('grp', 'ep')), parts along dimension 0, may hold values from 0.1 to 1
- w_gate: bfloat16 [32, 1024, 2048], P('ep', None, 'tp'), may hold values from -0.1875 to 0.1875
- w_up: bfloat16 [32, 1024, 2048], P('ep', None, 'tp'), may hold values from -0.1875 to 0.1875
- w_down: bfloat16 [32, 2048, 1024], P('ep', 'tp'), may hold values from -0.125 to 0.125
Outputs:
- mixed: bfloat16 [640, 1024], P(('grp', 'ep'), 'tp'), parts along dimension 0
- new_keys: bfloat16 [640, 512], P(('grp', 'ep'), 'tp'), parts along dimension 0
- new_values: bfloat16 [640, 512], P(('grp', 'ep'), 'tp'), parts along dimension 0
The draws below stay inside these ranges and needn't reach their ends.
There are 2 independent parts, one for each index of `grp`. The reference program is written for one: setup_inputs(seed, part) draws one part's arguments, and reference() takes and returns one part's arrays. A program takes and returns all parts, laid end to end along the dimension named above; an argument that names none is the same for every part. Nothing has to cross between parts.
Inputs may be any that keep to these rules, and one draw needn't show every extreme that they name: `route_ids`: each row names 2 different experts. In each aligned block of 10 rows no expert is named more than 2 times, and in some block some expert is named exactly 2 times.
All inputs are finite; a program needn't handle non-finite values.
Results may differ from the reference program's by a relative error of at most 0.012.
Values may be sent and summed in bfloat16 or wider, within the bound.
A program may use at most 64 MiB of HBM per device.

```python
import math
import jax
import jax.numpy as jnp
import numpy as np
from jax import lax

D = 1024
HEADS = 16
KV_HEADS = 8
HEAD_SIZE = 64
FF = 2048
TOPK = 2
SEQ_DEV = 10
CACHE_LEN = 1024
QDIM = 1024
KVDIM = 512
SEQS = 320
EXPERTS = 32
CAP = 2
N_EP = 32
N_TP = 8


def draw_tokens(key, part):
    base_key = jax.random.fold_in(key, 11)
    key_rows, key_cols, key_base = jax.random.split(base_key, 3)
    row_scale = jnp.exp(jax.random.uniform(key_rows, (SEQS, 1), jnp.float32, math.log(0.3), math.log(3.0)))
    position = jnp.arange(D, dtype=jnp.float32) / D - 0.5
    rough = jnp.exp(jax.random.uniform(key_cols, (1, D), jnp.float32, -0.35, 0.35))
    col_scale = jnp.exp(math.log(3.0) * position)[None, :] * rough
    base = jnp.clip(jax.random.normal(key_base, (SEQS, D), jnp.float32), -5.0, 5.0)
    return (base * row_scale * col_scale).astype(jnp.bfloat16)


def place_ends(drawn, stream_key, smallest, largest):
    index_at = [jax.random.randint(jax.random.fold_in(stream_key, axis), (), 0, length) for axis, length in enumerate(drawn.shape)]
    longest = drawn.shape.index(max(drawn.shape))
    beside = index_at[:longest] + [(index_at[longest] + 1) % drawn.shape[longest]] + index_at[longest + 1:]
    return drawn.at[tuple(index_at)].set(smallest).at[tuple(beside)].set(largest)


def level_of(own_key, shape, cuts, smallest, largest):
    def one(dim, parts):
        steps = jax.random.uniform(jax.random.fold_in(jax.random.fold_in(own_key, 6), dim), (parts,), jnp.float32, smallest / len(cuts), largest / len(cuts))
        return jnp.repeat(jnp.exp(steps), shape[dim] // parts).reshape((-1,) + (1,) * (len(shape) - dim - 1))

    level = one(*cuts[0])
    for cut in cuts[1:]:
        level = level * one(*cut)
    return level


def assign_block(own_key, own, number, rows, amount, top, limit, skew):
    sequence = jax.random.permutation(own_key, amount)
    heavy_load, usual = shares(amount, rows * top, limit, skew, True), shares(amount, rows * top, limit, skew, False)
    places = jnp.arange(amount)

    def named(sizes, rotation):
        used = int((sizes > 0).sum())
        fixed = max(1, used // 4)
        passed = fixed + (places - fixed + rotation * (used - fixed)) % max(1, amount - fixed)
        return jnp.zeros((amount,), jnp.int32).at[sequence[jnp.where(places < fixed, places, passed)]].set(jnp.asarray(sizes, jnp.int32))

    sizes = jnp.where(number % 4 == 0, named(heavy_load, number // 4), named(usual, number - number // 4 - 1))
    mixed = jax.random.permutation(jax.random.fold_in(own, 3), amount)
    source_of, receiver = mixed[0:amount // 2 * 2:2], mixed[1:amount // 2 * 2:2]
    room = jnp.minimum(sizes[source_of] - 1, limit - sizes[receiver]) // 2
    room = jnp.where((source_of == sequence[0]) | (receiver == sequence[0]) | (sizes[receiver] == 0), 0, jnp.maximum(room, 0))
    passed = jax.random.randint(jax.random.fold_in(own, 4), (amount // 2,), 0, 1 << 20) % (room + 1)
    sizes = sizes.at[source_of].add(-passed).at[receiver].add(passed)
    members = jnp.searchsorted(jnp.cumsum(sizes), jnp.arange(rows * top), side="right").astype(jnp.int32)
    grid = members.reshape(top, rows).T
    grid = grid[jax.random.permutation(jax.random.fold_in(own, 1), rows)]
    rotation = jax.random.randint(jax.random.fold_in(own, 2), (rows, 1), 0, top)
    return jnp.take_along_axis(grid, (jnp.arange(top)[None, :] + rotation) % top, axis=1)


def shares(number_of, total, reach, slope, full):
    loads = [(1 << 20) // math.isqrt(grade ** slope) + 1 for grade in range(1, number_of + 1)]
    largest = reach if full else min(reach, max(-(-total // number_of), total * loads[0] // sum(loads)))
    least = 1 if total - largest >= number_of - 1 else 0
    counts, surplus = [largest] + [least] * (number_of - 1), total - largest - least * (number_of - 1)
    while surplus > 0:
        candidates = [i for i in range(1, number_of) if counts[i] < largest] or [i for i in range(1, number_of) if counts[i] < reach]
        pool, budget = sum([loads[i] for i in candidates]), surplus
        for i in candidates:
            extra = min(reach - counts[i], max(1, budget * loads[i] // pool), surplus)
            counts[i] = counts[i] + extra
            surplus = surplus - extra
    return np.array(counts)


def scatter_about(rng, extent, spread, limit, shards=(), kind=jnp.bfloat16):
    level = level_of(rng, extent, shards, -0.22, 0.18) if shards else 1.0
    entries = jax.random.normal(rng, extent, jnp.float32) * spread * level
    return jnp.minimum(jnp.maximum(entries, -limit), limit).astype(kind)


def setup_inputs(seed: int = 0, part: int = 0) -> dict:
    keys = jax.random.split(jax.random.key(seed), 17)
    own_keys = jax.random.split(jax.random.fold_in(keys[16], part), 17)
    tokens = draw_tokens(jax.random.fold_in(jax.random.fold_in(keys[16], part), 71), part)
    attn_gain = jnp.clip(1.0 + 0.18 * jax.random.normal(keys[1], (D,), jnp.float32), 0.1, 1.9)
    w_query = scatter_about(keys[2], (D, QDIM), D ** -0.5, 0.1875, ((1, 8),))
    w_key = scatter_about(keys[3], (D, KVDIM), D ** -0.5, 0.1875, ((1, 8),))
    w_value = scatter_about(keys[4], (D, KVDIM), D ** -0.5, 0.1875, ((1, 8),))
    key_cache = scatter_about(own_keys[5], (SEQS, KVDIM, CACHE_LEN), 1.0, 6.0, ((0, 32), (1, 8)))
    value_cache = scatter_about(own_keys[6], (SEQS, KVDIM, CACHE_LEN), 1.0, 6.0, ((0, 32), (1, 8)))
    lengths = place_ends(jax.random.randint(own_keys[7], (SEQS,), CACHE_LEN // 4, CACHE_LEN + 1), jax.random.fold_in(own_keys[7], 1), CACHE_LEN // 4, CACHE_LEN).astype(jnp.int32)
    head_bias = jnp.clip(-8.0 + 6.0 * jax.random.uniform(keys[8], (HEADS,), jnp.float32) ** level_of(keys[8], (HEADS,), ((0, 8),), -0.2, 0.2), -8.0, -2.0)
    w_out = scatter_about(keys[9], (QDIM, D), QDIM ** -0.5, 0.1875, ((1, 8),))
    ffn_gain = jnp.clip(1.0 + 0.18 * jax.random.normal(keys[10], (D,), jnp.float32), 0.1, 1.9)
    route_ids_keys = jax.random.split(jax.random.fold_in(own_keys[11], 1), SEQS // SEQ_DEV)
    route_ids_turns = jax.random.permutation(jax.random.fold_in(own_keys[11], 3), SEQS // SEQ_DEV)
    route_ids = jax.vmap(lambda own, number: assign_block(jax.random.fold_in(own_keys[11], 2), own, number, SEQ_DEV, EXPERTS, TOPK, CAP, 2))(route_ids_keys, route_ids_turns).reshape((SEQS, TOPK))
    route_weights = jnp.clip(0.1 + 0.9 * jax.random.uniform(own_keys[12], (SEQS, TOPK), jnp.float32) ** level_of(own_keys[12], (SEQS, TOPK), ((0, 32),), -0.2, 0.2), 0.1, 1.0)
    w_gate = scatter_about(keys[13], (EXPERTS, D, FF), D ** -0.5, 0.1875, ((0, 32), (2, 8)))
    w_up = scatter_about(keys[14], (EXPERTS, D, FF), D ** -0.5, 0.1875, ((0, 32), (2, 8)))
    w_down = scatter_about(keys[15], (EXPERTS, FF, D), FF ** -0.5, 0.125, ((0, 32), (1, 8)))
    return {"tokens": tokens, "attn_gain": attn_gain, "w_query": w_query, "w_key": w_key, "w_value": w_value, "key_cache": key_cache, "value_cache": value_cache, "lengths": lengths, "head_bias": head_bias, "w_out": w_out, "ffn_gain": ffn_gain, "route_ids": route_ids, "route_weights": route_weights, "w_gate": w_gate, "w_up": w_up, "w_down": w_down}


epsilon = 1e-06

def rms_rows(values, gain):
    mean_sq = lax.optimization_barrier(jnp.mean(values * values, axis=-1, keepdims=True))
    return values * lax.rsqrt(mean_sq + epsilon) * gain

def attend_one(queries, key_block, value_block, length, head_shift):
    group_size = HEADS // KV_HEADS
    query_heads = queries.astype(jnp.float32).reshape(KV_HEADS, group_size, HEAD_SIZE)
    key_heads = key_block.astype(jnp.float32).reshape(KV_HEADS, HEAD_SIZE, CACHE_LEN)
    value_heads = value_block.astype(jnp.float32).reshape(KV_HEADS, HEAD_SIZE, CACHE_LEN)
    scores = jnp.einsum('kgd,kdl->kgl', query_heads, key_heads) * HEAD_SIZE ** (-0.5)
    scores = scores + head_shift.reshape(KV_HEADS, group_size)[:, :, None]
    in_cache = jnp.arange(CACHE_LEN, dtype=jnp.int32)[None, None, :] < length
    log_rest = jnp.where(in_cache, jax.nn.log_sigmoid(-scores), 0.0)
    tail_sum = lax.cumsum(log_rest, axis=2, reverse=True) - log_rest
    breaks = jnp.where(in_cache, jnp.exp(jax.nn.log_sigmoid(scores) + tail_sum), 0.0).astype(jnp.bfloat16)
    heads_out = jnp.einsum('kgl,kdl->kgd', breaks.astype(jnp.float32), value_heads)
    return heads_out.reshape(QDIM).astype(jnp.bfloat16)

def reference(tokens, attn_gain, w_query, w_key, w_value, key_cache, value_cache, lengths, head_bias, w_out, ffn_gain, route_ids, route_weights, w_gate, w_up, w_down):
    token_rows = tokens.astype(jnp.float32)
    normed = rms_rows(token_rows, attn_gain).astype(jnp.bfloat16)
    queries = jnp.dot(normed, w_query, preferred_element_type=jnp.float32).astype(jnp.bfloat16)
    new_keys = jnp.dot(normed, w_key, preferred_element_type=jnp.float32).astype(jnp.bfloat16)
    new_values = jnp.dot(normed, w_value, preferred_element_type=jnp.float32).astype(jnp.bfloat16)

    def per_sequence(items):
        return attend_one(items[0], items[1], items[2], items[3], head_bias)
    heads_out = lax.map(per_sequence, (queries, key_cache, value_cache, lengths))
    attn_out = jnp.dot(heads_out, w_out, preferred_element_type=jnp.float32)
    hidden = token_rows + attn_out
    ffn_in = rms_rows(hidden, ffn_gain).astype(jnp.bfloat16)
    pair_expert = route_ids.reshape(-1)
    pair_weight = route_weights.reshape(-1)
    most_rows = N_EP * CAP

    def one_expert(running, expert):
        matches = pair_expert == expert
        pair_order = jnp.argsort(jnp.where(matches, 0, 1).astype(jnp.int32), stable=True)[:most_rows]
        is_live = matches[pair_order]
        token_index = (pair_order // TOPK).astype(jnp.int32)
        chosen = jnp.where(is_live[:, None], ffn_in[token_index], jnp.zeros((), jnp.bfloat16))
        gate_act = jnp.dot(chosen, w_gate[expert], preferred_element_type=jnp.float32)
        up_act = jnp.dot(chosen, w_up[expert], preferred_element_type=jnp.float32)
        hidden_act = (jax.nn.silu(gate_act) * up_act).astype(jnp.bfloat16)
        inner_groups = hidden_act.astype(jnp.float32).reshape(most_rows, N_TP, FF // N_TP)
        down_groups = w_down[expert].astype(jnp.float32).reshape(N_TP, FF // N_TP, D)
        group_terms = jnp.einsum('rgf,gfd->rgd', inner_groups, down_groups).astype(jnp.bfloat16)
        result = lax.optimization_barrier(jnp.sum(group_terms.astype(jnp.float32), axis=1)).astype(jnp.bfloat16)
        pair_scale = jnp.where(is_live, pair_weight[pair_order], 0.0)
        running = running.at[token_index].add(result.astype(jnp.float32) * pair_scale[:, None])
        return (running, None)
    routed_sum, _ = lax.scan(one_expert, jnp.zeros((SEQS, D), jnp.float32), jnp.arange(EXPERTS, dtype=jnp.int32))
    mixed = (hidden + routed_sum).astype(jnp.bfloat16)
    return (mixed, new_keys, new_values)
```

```python
import functools

import jax
import jax.numpy as jnp
from jax import lax
from jax.experimental import pallas as pl
from jax.experimental.pallas import tpu as pltpu
from jax.sharding import PartitionSpec as P

HEAD_SIZE = 64
LANES = 128
CORES = 2
epsilon = 1e-06
f32 = jnp.float32
bf16 = jnp.bfloat16


def iota(shape, dim):
    return lax.broadcasted_iota(jnp.int32, shape, dim)


def hops(step, count):
    return min(step % count, -step % count)


def far_first(count):
    return sorted(range(1, count), key=lambda step: -hops(step, count))


def near_first(count):
    return sorted(range(1, count), key=lambda step: hops(step, count))


def nt_dot(left, right):
    return lax.dot_general(left, right, (((1,), (1,)), ((), ())), preferred_element_type=f32)


def kernel(
    n_tp,
    n_ep,
    tok_hbm,
    again_hbm,
    wq_hbm,
    wk_hbm,
    wv_hbm,
    key_hbm,
    val_hbm,
    len_hbm,
    bias_hbm,
    wo_hbm,
    fgain_hbm,
    ids_hbm,
    rw_hbm,
    wg_hbm,
    wu_hbm,
    wd_hbm,
    mixed_ref,
    nk_ref,
    nv_ref,
    tok,
    again,
    wq,
    wk,
    wv,
    key,
    val,
    lens,
    bias,
    wo,
    fgain,
    ids,
    rw,
    wg,
    wu,
    wd,
    rows_pad,
    idp,
    rwp,
    tri,
    place,
    combine,
    hid,
    hg,
    zsend,
    xg,
    rsend,
    rrecv,
    ysend,
    ret,
    local_sem,
    h_ssem,
    h_rsem,
    z_ssem,
    z_rsem,
    g_ssem,
    g_rsem,
    r_ssem,
    r_rsem,
    y_ssem,
    y_rsem,
):
    tp = lax.axis_index("tp")
    ep = lax.axis_index("ep")
    core = lax.rem(ep, CORES)
    chip = ep // CORES
    chips = n_ep // CORES
    half = n_ep // 2
    seq_rows = tok.shape[0]
    slots = 2 * n_ep

    barrier = pltpu.get_barrier_semaphore()
    for step in far_first(n_tp):
        pl.semaphore_signal(barrier, inc=1, device_id={"tp": lax.rem(tp + step, n_tp)})

    @pl.loop(1, n_ep)
    def _(step):
        pl.semaphore_signal(barrier, inc=1, device_id={"ep": lax.rem(ep + step, n_ep)})

    pairs = (
        (tok_hbm, tok),
        (again_hbm, again),
        (wq_hbm, wq),
        (len_hbm, lens),
        (bias_hbm, bias),
        (key_hbm, key),
        (ids_hbm, ids),
        (rw_hbm, rw),
        (val_hbm, val),
        (wo_hbm, wo),
        (fgain_hbm, fgain),
        (wk_hbm, wk),
        (wv_hbm, wv),
        (wg_hbm, wg),
        (wu_hbm, wu),
        (wd_hbm, wd),
    )
    copies = [
        pltpu.make_async_copy(source, target, local_sem.at[number])
        for number, (source, target) in enumerate(pairs)
    ]
    for copy in copies:
        copy.start()
    (
        c_tok, c_again, c_wq, c_len, c_bias, c_key, c_ids, c_rw,
        c_val, c_wo, c_fgain, c_wk, c_wv, c_wg, c_wu, c_wd,
    ) = copies

    def landed(view, sem):
        pltpu.make_async_copy(view, view, sem).wait()

    tri_len = tri.shape[0]
    tri[...] = (iota((tri_len, tri_len), 0) > iota((tri_len, tri_len), 1)).astype(f32).astype(bf16)
    rows_pad[...] = jnp.zeros_like(rows_pad)
    hid[...] = jnp.zeros_like(hid)
    idp[...] = jnp.full(idp.shape, -1.0, f32)
    rwp[...] = jnp.zeros_like(rwp)

    c_tok.wait()
    c_again.wait()
    token_rows = tok[...].astype(f32)
    mean_sq = jnp.mean(token_rows * token_rows, axis=1, keepdims=True)
    normed = (token_rows * lax.rsqrt(mean_sq + epsilon) * again[...]).astype(bf16)
    c_wq.wait()
    queries = jnp.dot(normed, wq[...], preferred_element_type=f32).astype(bf16).astype(f32)
    rows_pad[pl.ds(0, seq_rows), :] = queries * HEAD_SIZE ** (-0.5)
    padded = rows_pad[...]
    pad_rows = padded.shape[0]
    low = iota(padded.shape, 1) < HEAD_SIZE
    turned = pltpu.roll(padded, HEAD_SIZE, axis=1)
    both = jnp.concatenate([jnp.where(low, padded, turned), jnp.where(low, turned, padded)], axis=0)
    cols = key.shape[0]
    wide = jnp.concatenate([both] * (cols // LANES), axis=1)
    own_block = (iota(wide.shape, 1) // HEAD_SIZE) == lax.rem(iota(wide.shape, 0), pad_rows)
    spread = jnp.where(own_block, wide, 0.0).astype(bf16)

    c_len.wait()
    c_bias.wait()
    idp[pl.ds(2, 1), pl.ds(0, seq_rows)] = lens[...].astype(f32)
    len_row = jnp.broadcast_to(idp[pl.ds(2, 1), :], (2 * pad_rows, LANES))
    own_lane = iota(len_row.shape, 1) == lax.rem(iota(len_row.shape, 0), pad_rows)
    len_col = jnp.sum(jnp.where(own_lane, len_row, 0.0), axis=1, keepdims=True)
    bias_col = jnp.where(
        iota((2 * pad_rows, 1), 0) < pad_rows, bias[pl.ds(0, 1), pl.ds(0, 1)], bias[pl.ds(0, 1), pl.ds(1, 1)]
    )

    c_key.wait()
    scores = jnp.dot(spread, key[...], preferred_element_type=f32) + bias_col
    in_cache = iota(scores.shape, 1).astype(f32) < len_col
    log_rest = -(jnp.maximum(scores, 0.0) + jnp.log1p(jnp.exp(-jnp.abs(scores))))
    log_rest = jnp.where(in_cache, log_rest, 0.0)
    cache_len = scores.shape[1]
    chunk_count = cache_len // tri_len
    high = log_rest.astype(bf16)
    rest = (log_rest - high.astype(f32)).astype(bf16)
    stacked = jnp.concatenate(
        [part[:, c * tri_len : (c + 1) * tri_len] for part in (high, rest) for c in range(chunk_count)], axis=0
    )
    within = jnp.dot(stacked, tri[...], preferred_element_type=f32)
    tails = []
    carry = jnp.zeros((2 * pad_rows, 1), f32)
    span = 2 * pad_rows
    for c in reversed(range(chunk_count)):
        inner = within[c * span : (c + 1) * span] + within[(chunk_count + c) * span : (chunk_count + c + 1) * span]
        tails.append(inner + carry)
        carry = carry + inner[:, 0:1] + log_rest[:, c * tri_len : c * tri_len + 1]
    tail = jnp.concatenate(tails[::-1], axis=1)
    breaks = jnp.where(in_cache, jnp.exp(scores + log_rest + tail), 0.0).astype(bf16)
    c_val.wait()
    mixed_values = nt_dot(breaks, val[...])
    mixed_values = jnp.where(own_block, mixed_values, 0.0)
    folded = mixed_values[:, 0:LANES]
    for c in range(1, cols // LANES):
        folded = folded + mixed_values[:, c * LANES : (c + 1) * LANES]
    folded = folded + pltpu.roll(folded, HEAD_SIZE, axis=1)
    heads = jnp.where(low, folded[:pad_rows], folded[pad_rows:]).astype(bf16)
    hg[tp] = heads

    pl.semaphore_wait(barrier, (n_tp - 1) + (n_ep - 1))
    sends = []
    for step in far_first(n_tp):
        copy = pltpu.make_async_remote_copy(
            hg.at[tp], hg.at[tp], h_ssem.at[step], h_rsem.at[tp], device_id={"tp": lax.rem(tp + step, n_tp)}
        )
        copy.start()
        sends.append(copy)

    c_wk.wait()
    c_wv.wait()
    nk_ref[...] = nt_dot(normed, wk[...]).astype(bf16)
    nv_ref[...] = nt_dot(normed, wv[...]).astype(bf16)
    c_ids.wait()
    c_rw.wait()
    top_count = ids.shape[0]
    idp[pl.ds(0, top_count), pl.ds(0, seq_rows)] = ids[...].astype(f32)
    rwp[pl.ds(0, top_count), pl.ds(0, seq_rows)] = rw[...]
    slot_expert = (iota((slots, LANES), 0) // 2).astype(f32)
    slot_rank = lax.rem(iota((slots, LANES), 0), 2).astype(f32)
    hits = [(slot_expert == idp[pl.ds(k, 1), :]).astype(f32) for k in range(top_count)]
    any_hit = sum(hits)
    upper = (iota((LANES, LANES), 0) < iota((LANES, LANES), 1)).astype(f32).astype(bf16)
    before = jnp.dot(any_hit.astype(bf16), upper, preferred_element_type=f32)
    taken = jnp.where(before == slot_rank, 1.0, 0.0)
    place[...] = (any_hit * taken).astype(bf16)
    weighted = sum(hits[k] * rwp[pl.ds(k, 1), :] for k in range(top_count)) * taken
    weighted_t = weighted.T[: combine.shape[0] // 2]
    weighted_high = weighted_t.astype(bf16)
    combine[pl.ds(0, pad_rows), :] = weighted_high
    combine[pl.ds(pad_rows, pad_rows), :] = (weighted_t - weighted_high.astype(f32)).astype(bf16)
    c_fgain.wait()
    own_cols = pl.ds(pl.multiple_of(tp * LANES, LANES), LANES)
    own_tokens = tok[:, own_cols].astype(f32)
    own_gain = fgain[:, own_cols]

    c_wo.wait()
    attn_out = jnp.dot(hg[tp], wo[own_cols, :], preferred_element_type=f32)
    for step in near_first(n_tp):
        peer = lax.rem(tp + step, n_tp)
        landed(hg.at[peer], h_rsem.at[peer])
        attn_out += jnp.dot(
            hg[peer], wo[pl.ds(pl.multiple_of(peer * LANES, LANES), LANES), :], preferred_element_type=f32
        )
    hid[pl.ds(0, seq_rows), :] = own_tokens + attn_out[:seq_rows]
    scaled = (hid[...] * own_gain).astype(bf16)
    outgoing = jnp.dot(place[...], scaled, preferred_element_type=f32).astype(bf16)
    zsend[...] = outgoing.reshape(zsend.shape)

    for step in far_first(chips):
        for to_core in range(CORES):
            to_ep = lax.rem(chip + step, chips) * CORES + to_core
            at = ((chips - step + chips // 4 - 1) % chips) * CORES + core
            copy = pltpu.make_async_remote_copy(
                zsend.at[to_ep],
                xg.at[tp, at],
                z_ssem.at[step * CORES + to_core],
                z_rsem.at[at],
                device_id={"ep": to_ep},
            )
            copy.start()
            sends.append(copy)
    home = (chips // 4 - 1) * CORES
    partner = chip * CORES + (1 - core)
    copy = pltpu.make_async_remote_copy(
        zsend.at[partner], xg.at[tp, home + core], z_ssem.at[0], z_rsem.at[home + core], device_id={"ep": partner}
    )
    copy.start()
    sends.append(copy)
    xg[tp, home + core] = zsend[ep]

    for part in range(2):
        for number in range(half):
            at = part * half + number
            if at // CORES == home // CORES:
                continue
            landed(xg.at[tp, at], z_rsem.at[at])
        if part == 0:
            landed(xg.at[tp, home + 1 - core], z_rsem.at[home + 1 - core])
        span_at = pl.ds(part * half, half)
        for step in far_first(n_tp):
            copy = pltpu.make_async_remote_copy(
                xg.at[tp, span_at],
                xg.at[tp, span_at],
                g_ssem.at[part, step],
                g_rsem.at[part, tp],
                device_id={"tp": lax.rem(tp + step, n_tp)},
            )
            copy.start()
            sends.append(copy)

    c_wg.wait()
    c_wu.wait()
    c_wd.wait()
    gate = jnp.zeros((slots, wg.shape[1]), f32)
    up = jnp.zeros((slots, wu.shape[1]), f32)
    sum_sq = jnp.zeros((slots, 1), f32)
    for step in [0] + near_first(n_tp):
        peer = lax.rem(tp + step, n_tp)
        if step:
            for part in range(2):
                landed(xg.at[peer, pl.ds(part * half, half)], g_rsem.at[part, peer])
        rows = xg[peer].reshape(slots, LANES)
        peer_cols = pl.ds(pl.multiple_of(peer * LANES, LANES), LANES)
        gate += jnp.dot(rows, wg[peer_cols, :], preferred_element_type=f32)
        up += jnp.dot(rows, wu[peer_cols, :], preferred_element_type=f32)
        plain = rows.astype(f32) / fgain[:, peer_cols]
        sum_sq += jnp.sum(plain * plain, axis=1, keepdims=True)
    scale = lax.rsqrt(sum_sq / (n_tp * LANES) + epsilon)
    gate = gate * scale
    up = up * scale
    hidden_act = (gate / (1.0 + jnp.exp(-gate)) * up).astype(bf16)
    for part in (1, 0):
        act = hidden_act[part * slots // 2 : (part + 1) * slots // 2]
        partial_value = jnp.dot(act, wd[...], preferred_element_type=f32).astype(bf16)
        for c in range(n_tp):
            rsend[part, c] = partial_value[:, c * LANES : (c + 1) * LANES]
        for step in far_first(n_tp):
            peer = lax.rem(tp + step, n_tp)
            copy = pltpu.make_async_remote_copy(
                rsend.at[part, peer],
                rrecv.at[part, tp],
                r_ssem.at[part, step],
                r_rsem.at[part, tp],
                device_id={"tp": peer},
            )
            copy.start()
            sends.append(copy)

    for part in (1, 0):
        total = rsend[part, tp].astype(f32)
        for step in near_first(n_tp):
            peer = lax.rem(tp + step, n_tp)
            landed(rrecv.at[part, peer], r_rsem.at[part, peer])
            total += rrecv[part, peer].astype(f32)
        span_at = pl.ds(part * half, half)
        ysend[span_at] = total.astype(bf16).reshape(half, 2, LANES)
        order = range(half * part, half * (part + 1))
        order = sorted(order, key=lambda at: -hops((at - home) // CORES, chips))
        for at in order:
            step = at // CORES - home // CORES
            if step == 0:
                continue
            to_ep = lax.rem(chip + step + chips, chips) * CORES + at % CORES
            copy = pltpu.make_async_remote_copy(
                ysend.at[at], ret.at[ep], y_ssem.at[at], y_rsem.at[ep], device_id={"ep": to_ep}
            )
            copy.start()
            sends.append(copy)
        if part == 0:
            copy = pltpu.make_async_remote_copy(
                ysend.at[home + 1 - core], ret.at[ep], y_ssem.at[home], y_rsem.at[ep], device_id={"ep": partner}
            )
            copy.start()
            sends.append(copy)
            ret[ep] = ysend[home + core]

    for step in near_first(chips):
        for from_core in range(CORES):
            from_ep = lax.rem(chip + step, chips) * CORES + from_core
            landed(ret.at[from_ep], y_rsem.at[from_ep])
    landed(ret.at[partner], y_rsem.at[partner])
    picked = jnp.dot(combine[...], ret[...].reshape(slots, LANES), preferred_element_type=f32)
    routed_sum = picked[:pad_rows] + picked[pad_rows:]
    mixed_ref[...] = (hid[pl.ds(0, seq_rows), :] + routed_sum[:seq_rows]).astype(bf16)
    for copy in sends:
        copy.wait_send()


def shards(
    n_tp,
    n_ep,
    tokens,
    attn_gain,
    w_query,
    w_key,
    w_value,
    key_cache,
    value_cache,
    lengths,
    head_bias,
    w_out,
    ffn_gain,
    route_ids,
    route_weights,
    w_gate,
    w_up,
    w_down,
):
    seq_rows, model_width = tokens.shape
    cache_len = key_cache.shape[2]
    kv_cols = key_cache.shape[1]
    pad_rows = 16
    slots = 2 * n_ep
    operands = (
        tokens,
        attn_gain.reshape(1, model_width),
        w_query,
        w_key.T,
        w_value.T,
        key_cache.reshape(seq_rows * kv_cols, cache_len),
        value_cache.reshape(seq_rows * kv_cols, cache_len),
        lengths.reshape(1, seq_rows),
        head_bias.reshape(1, head_bias.shape[0]),
        w_out,
        ffn_gain.reshape(1, model_width),
        route_ids.T,
        route_weights.T,
        w_gate[0],
        w_up[0],
        w_down[0],
    )
    dma = pltpu.SemaphoreType.DMA
    scratch = [pltpu.VMEM(op.shape, op.dtype) for op in operands] + [
        pltpu.VMEM((pad_rows, LANES), f32),
        pltpu.VMEM((8, LANES), f32),
        pltpu.VMEM((8, LANES), f32),
        pltpu.VMEM((256, 256), bf16),
        pltpu.VMEM((slots, LANES), bf16),
        pltpu.VMEM((2 * pad_rows, slots), bf16),
        pltpu.VMEM((LANES, LANES), f32),
        pltpu.VMEM((n_tp, pad_rows, LANES), bf16),
        pltpu.VMEM((n_ep, 2, LANES), bf16),
        pltpu.VMEM((n_tp, n_ep, 2, LANES), bf16),
        pltpu.VMEM((2, n_tp, slots // 2, LANES), bf16),
        pltpu.VMEM((2, n_tp, slots // 2, LANES), bf16),
        pltpu.VMEM((n_ep, 2, LANES), bf16),
        pltpu.VMEM((n_ep, 2, LANES), bf16),
        dma((len(operands),)),
        dma((n_tp,)),
        dma((n_tp,)),
        dma((n_ep,)),
        dma((n_ep,)),
        dma((2, n_tp)),
        dma((2, n_tp)),
        dma((2, n_tp)),
        dma((2, n_tp)),
        dma((n_ep,)),
        dma((n_ep,)),
    ]
    return pl.pallas_call(
        functools.partial(kernel, n_tp, n_ep),
        out_shape=(
            jax.ShapeDtypeStruct((seq_rows, w_out.shape[1]), bf16),
            jax.ShapeDtypeStruct((seq_rows, w_key.shape[1]), bf16),
            jax.ShapeDtypeStruct((seq_rows, w_value.shape[1]), bf16),
        ),
        in_specs=[pl.BlockSpec(memory_space=pltpu.HBM)] * len(operands),
        out_specs=[pl.BlockSpec(memory_space=pltpu.VMEM)] * 3,
        scratch_shapes=scratch,
        compiler_params=pltpu.CompilerParams(collective_id=0, has_side_effects=True),
    )(*operands)


def solution(mesh):
    in_specs = (
        P(("grp", "ep"), None),
        P(),
        P(None, "tp"),
        P(None, "tp"),
        P(None, "tp"),
        P(("grp", "ep"), "tp", None),
        P(("grp", "ep"), "tp", None),
        P(("grp", "ep")),
        P("tp"),
        P(None, "tp"),
        P(),
        P(("grp", "ep"), None),
        P(("grp", "ep"), None),
        P("ep", None, "tp"),
        P("ep", None, "tp"),
        P("ep", "tp", None),
    )
    out_specs = (P(("grp", "ep"), "tp"), P(("grp", "ep"), "tp"), P(("grp", "ep"), "tp"))
    body = functools.partial(shards, mesh.shape["tp"], mesh.shape["ep"])
    return jax.shard_map(body, mesh=mesh, in_specs=in_specs, out_specs=out_specs, check_vma=False)
```

```python
import functools

import jax
import jax.numpy as jnp
from jax import lax
from jax.experimental import pallas as pl
from jax.experimental.pallas import tpu as pltpu
from jax.sharding import PartitionSpec as P

HEAD_SIZE = 64
LANES = 128
CORES = 2
epsilon = 1e-06
f32 = jnp.float32
bf16 = jnp.bfloat16


def iota(shape, dim):
    return lax.broadcasted_iota(jnp.int32, shape, dim)


def hops(step, count):
    return min(step % count, -step % count)


def far_first(count):
    return sorted(range(1, count), key=lambda step: -hops(step, count))


def near_first(count):
    return sorted(range(1, count), key=lambda step: hops(step, count))


def at_part(step, count):
    return (count - step + count // 4 - 1) % count < count // 2


def nt_dot(left, right):
    return lax.dot_general(left, right, (((1,), (1,)), ((), ())), preferred_element_type=f32)


def kernel(
    n_tp,
    n_ep,
    tok_hbm,
    again_hbm,
    wq_hbm,
    wk_hbm,
    wv_hbm,
    key_hbm,
    val_hbm,
    len_hbm,
    bias_hbm,
    wo_hbm,
    fgain_hbm,
    ids_hbm,
    rw_hbm,
    wg_hbm,
    wu_hbm,
    wd_hbm,
    mixed_ref,
    nk_ref,
    nv_ref,
    tok,
    again,
    wq,
    wk,
    wv,
    key,
    val,
    lens,
    bias,
    wo,
    fgain,
    ids,
    rw,
    wg,
    wu,
    wd,
    rows_pad,
    idp,
    rwp,
    tri,
    place,
    combine,
    hid,
    hg,
    zsend,
    zrecv,
    xg,
    rsend,
    rrecv,
    ysend,
    ret,
    local_sem,
    h_ssem,
    h_rsem,
    z_ssem,
    z_rsem,
    g_ssem,
    g_rsem,
    r_ssem,
    r_rsem,
    y_ssem,
    y_rsem,
):
    tp = lax.axis_index("tp")
    ep = lax.axis_index("ep")
    core = lax.rem(ep, CORES)
    chip = ep // CORES
    chips = n_ep // CORES
    half = n_ep // 2
    seq_rows = tok.shape[0]
    slots = 2 * n_ep

    def copies_of(first, pairs):
        made = [
            pltpu.make_async_copy(source, target, local_sem.at[first + number])
            for number, (source, target) in enumerate(pairs)
        ]
        for copy in made:
            copy.start()
        return made

    c_tok, c_again, c_wq, c_len, c_bias, c_key, c_val = copies_of(
        0,
        (
            (tok_hbm, tok),
            (again_hbm, again),
            (wq_hbm, wq),
            (len_hbm, lens),
            (bias_hbm, bias),
            (key_hbm, key),
            (val_hbm, val),
        ),
    )

    def wrap(number, count):
        return jnp.where(number >= count, number - count, number)

    barrier = pltpu.get_barrier_semaphore()
    for step in far_first(n_tp):
        pl.semaphore_signal(barrier, inc=1, device_id={"tp": wrap(tp + step, n_tp)})

    @pl.loop(1, n_ep)
    def _(step):
        pl.semaphore_signal(barrier, inc=1, device_id={"ep": wrap(ep + step, n_ep)})

    def landed(view, sem):
        pltpu.make_async_copy(view, view, sem).wait()

    tri_len = tri.shape[0]
    tri[...] = (iota((tri_len, tri_len), 0) > iota((tri_len, tri_len), 1)).astype(f32).astype(bf16)
    rows_pad[...] = jnp.zeros_like(rows_pad)
    hid[...] = jnp.zeros_like(hid)
    idp[...] = jnp.full(idp.shape, -1.0, f32)
    rwp[...] = jnp.zeros_like(rwp)

    c_tok.wait()
    c_again.wait()
    token_rows = tok[...].astype(f32)
    mean_sq = jnp.mean(token_rows * token_rows, axis=1, keepdims=True)
    normed = (token_rows * lax.rsqrt(mean_sq + epsilon) * again[...]).astype(bf16)
    c_wq.wait()
    queries = jnp.dot(normed, wq[...], preferred_element_type=f32).astype(bf16).astype(f32)
    rows_pad[pl.ds(0, seq_rows), :] = queries * HEAD_SIZE ** (-0.5)
    padded = rows_pad[...]
    pad_rows = padded.shape[0]
    low = iota(padded.shape, 1) < HEAD_SIZE
    turned = pltpu.roll(padded, HEAD_SIZE, axis=1)
    both = jnp.concatenate([jnp.where(low, padded, turned), jnp.where(low, turned, padded)], axis=0)
    cols = key.shape[0]
    wide = jnp.concatenate([both] * (cols // LANES), axis=1)
    own_block = (iota(wide.shape, 1) // HEAD_SIZE) == lax.rem(iota(wide.shape, 0), pad_rows)
    spread = jnp.where(own_block, wide, 0.0).astype(bf16)

    c_len.wait()
    c_bias.wait()
    idp[pl.ds(2, 1), pl.ds(0, seq_rows)] = lens[...].astype(f32)
    len_row = jnp.broadcast_to(idp[pl.ds(2, 1), :], (2 * pad_rows, LANES))
    own_lane = iota(len_row.shape, 1) == lax.rem(iota(len_row.shape, 0), pad_rows)
    len_col = jnp.sum(jnp.where(own_lane, len_row, 0.0), axis=1, keepdims=True)
    bias_col = jnp.where(
        iota((2 * pad_rows, 1), 0) < pad_rows, bias[pl.ds(0, 1), pl.ds(0, 1)], bias[pl.ds(0, 1), pl.ds(1, 1)]
    )

    c_key.wait()
    c_wo, c_wk, c_wv, c_ids, c_rw, c_fgain = copies_of(
        7, ((wo_hbm, wo), (wk_hbm, wk), (wv_hbm, wv), (ids_hbm, ids), (rw_hbm, rw), (fgain_hbm, fgain))
    )
    scores = jnp.dot(spread, key[...], preferred_element_type=f32) + bias_col
    in_cache = iota(scores.shape, 1).astype(f32) < len_col
    log_rest = -(jnp.maximum(scores, 0.0) + jnp.log1p(jnp.exp(-jnp.abs(scores))))
    log_rest = jnp.where(in_cache, log_rest, 0.0)
    cache_len = scores.shape[1]
    chunk_count = cache_len // tri_len
    high = log_rest.astype(bf16)
    rest = (log_rest - high.astype(f32)).astype(bf16)
    stacked = jnp.concatenate(
        [part[:, c * tri_len : (c + 1) * tri_len] for part in (high, rest) for c in range(chunk_count)], axis=0
    )
    within = jnp.dot(stacked, tri[...], preferred_element_type=f32)
    tails = []
    carry = jnp.zeros((2 * pad_rows, 1), f32)
    span = 2 * pad_rows
    for c in reversed(range(chunk_count)):
        inner = within[c * span : (c + 1) * span] + within[(chunk_count + c) * span : (chunk_count + c + 1) * span]
        tails.append(inner + carry)
        carry = carry + inner[:, 0:1] + log_rest[:, c * tri_len : c * tri_len + 1]
    tail = jnp.concatenate(tails[::-1], axis=1)
    breaks = jnp.where(in_cache, jnp.exp(scores + log_rest + tail), 0.0).astype(bf16)
    c_val.wait()
    mixed_values = nt_dot(breaks, val[...])
    mixed_values = jnp.where(own_block, mixed_values, 0.0)
    folded = mixed_values[:, 0:LANES]
    for c in range(1, cols // LANES):
        folded = folded + mixed_values[:, c * LANES : (c + 1) * LANES]
    folded = folded + pltpu.roll(folded, HEAD_SIZE, axis=1)
    heads = jnp.where(low, folded[:pad_rows], folded[pad_rows:]).astype(bf16)
    hg[tp] = heads

    pl.semaphore_wait(barrier, (n_tp - 1) + (n_ep - 1))
    for step in far_first(n_tp):
        pltpu.make_async_remote_copy(
            hg.at[tp], hg.at[tp], h_ssem, h_rsem, device_id={"tp": wrap(tp + step, n_tp)}
        ).start()

    c_wg, c_wu, c_wd = copies_of(0, ((wg_hbm, wg), (wu_hbm, wu), (wd_hbm, wd)))
    c_wk.wait()
    c_wv.wait()
    nk_ref[...] = nt_dot(normed, wk[...]).astype(bf16)
    nv_ref[...] = nt_dot(normed, wv[...]).astype(bf16)
    c_ids.wait()
    c_rw.wait()
    top_count = ids.shape[0]
    idp[pl.ds(0, top_count), pl.ds(0, seq_rows)] = ids[...].astype(f32)
    rwp[pl.ds(0, top_count), pl.ds(0, seq_rows)] = rw[...]
    slot_expert = (iota((slots, LANES), 0) // 2).astype(f32)
    slot_rank = lax.rem(iota((slots, LANES), 0), 2).astype(f32)
    hits = [(slot_expert == idp[pl.ds(k, 1), :]).astype(f32) for k in range(top_count)]
    any_hit = sum(hits)
    upper = (iota((LANES, LANES), 0) < iota((LANES, LANES), 1)).astype(f32).astype(bf16)
    before = jnp.dot(any_hit.astype(bf16), upper, preferred_element_type=f32)
    taken = jnp.where(before == slot_rank, 1.0, 0.0)
    place[...] = (any_hit * taken).astype(bf16)
    weighted = sum(hits[k] * rwp[pl.ds(k, 1), :] for k in range(top_count)) * taken
    weighted_t = weighted.T[: combine.shape[0] // 2]
    weighted_high = weighted_t.astype(bf16)
    combine[pl.ds(0, pad_rows), :] = weighted_high
    combine[pl.ds(pad_rows, pad_rows), :] = (weighted_t - weighted_high.astype(f32)).astype(bf16)
    c_fgain.wait()
    own_cols = pl.ds(pl.multiple_of(tp * LANES, LANES), LANES)
    own_tokens = tok[:, own_cols].astype(f32)
    own_gain = fgain[:, own_cols]

    c_wo.wait()
    inverse_sq = 1.0 / (fgain[...] * fgain[...])
    peers = pl.ds(0, n_tp - 1)
    landed(hg.at[peers], h_rsem)
    all_heads = jnp.concatenate([hg[peer] for peer in range(n_tp)], axis=1)
    attn_out = jnp.dot(all_heads, wo[...], preferred_element_type=f32)
    hid[pl.ds(0, seq_rows), :] = own_tokens + attn_out[:seq_rows]
    scaled = (hid[...] * own_gain).astype(bf16)
    outgoing = jnp.dot(place[...], scaled, preferred_element_type=f32).astype(bf16)
    zsend[...] = outgoing.reshape(zsend.shape)

    home = (chips // 4 - 1) * CORES
    partner = chip * CORES + (1 - core)
    for step in far_first(chips) + [0]:
        to_chip = wrap(chip + step, chips)
        at = ((chips - step + chips // 4 - 1) % chips) * CORES + core
        part = 0 if at_part(step, chips) else 1
        for to_core in range(CORES):
            to_ep = to_chip * CORES + to_core if step else partner
            if step == 0 and to_core:
                continue
            pltpu.make_async_remote_copy(
                zsend.at[to_ep], zrecv.at[at], z_ssem, z_rsem.at[part], device_id={"ep": to_ep}
            ).start()
    zrecv[home + core] = zsend[ep]

    for part in range(2):
        landed(zrecv.at[pl.ds(part * half, half - 1 + part)], z_rsem.at[part])
        xg[part, tp] = zrecv[pl.ds(part * half, half)].reshape(slots // 2, LANES)
        for step in far_first(n_tp):
            pltpu.make_async_remote_copy(
                xg.at[part, tp],
                xg.at[part, tp],
                g_ssem.at[part],
                g_rsem.at[part],
                device_id={"tp": wrap(tp + step, n_tp)},
            ).start()

    c_wg.wait()
    c_wu.wait()
    c_wd.wait()
    for part in range(2):
        landed(xg.at[part, peers], g_rsem.at[part])
    rows = jnp.concatenate(
        [jnp.concatenate([xg[part, peer] for peer in range(n_tp)], axis=1) for part in range(2)], axis=0
    )
    gate = jnp.dot(rows, wg[...], preferred_element_type=f32)
    up = jnp.dot(rows, wu[...], preferred_element_type=f32)
    plain = rows.astype(f32)
    sum_sq = jnp.sum(plain * plain * inverse_sq, axis=1, keepdims=True)
    scale = lax.rsqrt(sum_sq / (n_tp * LANES) + epsilon)
    gate = gate * scale
    up = up * scale
    hidden_act = (gate / (1.0 + jnp.exp(-gate)) * up).astype(bf16)
    for part in (1, 0):
        act = hidden_act[part * slots // 2 : (part + 1) * slots // 2]
        partial_value = jnp.dot(act, wd[...], preferred_element_type=f32).astype(bf16)
        for c in range(n_tp):
            rsend[part, c] = partial_value[:, c * LANES : (c + 1) * LANES]
        for step in far_first(n_tp):
            peer = wrap(tp + step, n_tp)
            pltpu.make_async_remote_copy(
                rsend.at[part, peer], rrecv.at[part, tp], r_ssem.at[part], r_rsem.at[part], device_id={"tp": peer}
            ).start()
        rrecv[part, tp] = rsend[part, tp]

    for part in (1, 0):
        landed(rrecv.at[part, peers], r_rsem.at[part])
        total = rrecv[part, 0].astype(f32)
        for peer in range(1, n_tp):
            total += rrecv[part, peer].astype(f32)
        ysend[pl.ds(part * half, half)] = total.astype(bf16).reshape(half, 2, LANES)
        order = range(half * part, half * (part + 1))
        for at in sorted(order, key=lambda at: -hops((at - home) // CORES, chips)):
            step = at // CORES - home // CORES
            if step:
                to_ep = wrap(chip + step % chips, chips) * CORES + at % CORES
                pltpu.make_async_remote_copy(
                    ysend.at[at], ret.at[ep], y_ssem, y_rsem, device_id={"ep": to_ep}
                ).start()
        if part == 0:
            pltpu.make_async_remote_copy(
                ysend.at[home + 1 - core], ret.at[ep], y_ssem, y_rsem, device_id={"ep": partner}
            ).start()
            ret[ep] = ysend[home + core]

    landed(hg.at[peers], h_ssem)
    landed(zsend.at[pl.ds(0, n_ep - 1)], z_ssem)
    for part in range(2):
        landed(xg.at[part, peers], g_ssem.at[part])
        landed(rsend.at[part, peers], r_ssem.at[part])
    landed(ysend.at[pl.ds(0, n_ep - 1)], y_ssem)
    landed(ret.at[pl.ds(0, n_ep - 1)], y_rsem)
    picked = jnp.dot(combine[...], ret[...].reshape(slots, LANES), preferred_element_type=f32)
    routed_sum = picked[:pad_rows] + picked[pad_rows:]
    mixed_ref[...] = (hid[pl.ds(0, seq_rows), :] + routed_sum[:seq_rows]).astype(bf16)


def write_out(*refs):
    count = len(refs) // 2
    copies = [pltpu.make_async_copy(refs[n], refs[count + n], refs[-1].at[n]) for n in range(count)]
    for copy in copies:
        copy.start()
    for copy in copies:
        copy.wait()


def shards(
    n_tp,
    n_ep,
    tokens,
    attn_gain,
    w_query,
    w_key,
    w_value,
    key_cache,
    value_cache,
    lengths,
    head_bias,
    w_out,
    ffn_gain,
    route_ids,
    route_weights,
    w_gate,
    w_up,
    w_down,
):
    seq_rows, model_width = tokens.shape
    cache_len = key_cache.shape[2]
    kv_cols = key_cache.shape[1]
    pad_rows = 16
    slots = 2 * n_ep
    operands = (
        tokens,
        attn_gain.reshape(1, model_width),
        w_query,
        w_key.T,
        w_value.T,
        key_cache.reshape(seq_rows * kv_cols, cache_len),
        value_cache.reshape(seq_rows * kv_cols, cache_len),
        lengths.reshape(1, seq_rows),
        head_bias.reshape(1, head_bias.shape[0]),
        w_out,
        ffn_gain.reshape(1, model_width),
        route_ids.T,
        route_weights.T,
        w_gate[0],
        w_up[0],
        w_down[0],
    )
    dma = pltpu.SemaphoreType.DMA
    scratch = [pltpu.VMEM(op.shape, op.dtype) for op in operands] + [
        pltpu.VMEM((pad_rows, LANES), f32),
        pltpu.VMEM((8, LANES), f32),
        pltpu.VMEM((8, LANES), f32),
        pltpu.VMEM((256, 256), bf16),
        pltpu.VMEM((slots, LANES), bf16),
        pltpu.VMEM((2 * pad_rows, slots), bf16),
        pltpu.VMEM((LANES, LANES), f32),
        pltpu.VMEM((n_tp, pad_rows, LANES), bf16),
        pltpu.VMEM((n_ep, 2, LANES), bf16),
        pltpu.VMEM((n_ep, 2, LANES), bf16),
        pltpu.VMEM((2, n_tp, slots // 2, LANES), bf16),
        pltpu.VMEM((2, n_tp, slots // 2, LANES), bf16),
        pltpu.VMEM((2, n_tp, slots // 2, LANES), bf16),
        pltpu.VMEM((n_ep, 2, LANES), bf16),
        pltpu.VMEM((n_ep, 2, LANES), bf16),
        dma((13,)),
        dma,
        dma,
        dma,
        dma((2,)),
        dma((2,)),
        dma((2,)),
        dma((2,)),
        dma((2,)),
        dma,
        dma,
    ]
    shapes = (
        (seq_rows, w_out.shape[1]),
        (seq_rows, w_key.shape[1]),
        (seq_rows, w_value.shape[1]),
    )
    results = pl.pallas_call(
        functools.partial(kernel, n_tp, n_ep),
        out_shape=tuple(pltpu.VMEM(shape, bf16) for shape in shapes),
        in_specs=[pl.BlockSpec(memory_space=pltpu.HBM)] * len(operands),
        out_specs=[pl.BlockSpec(memory_space=pltpu.VMEM)] * 3,
        scratch_shapes=scratch,
        compiler_params=pltpu.CompilerParams(collective_id=0, has_side_effects=True),
    )(*operands)
    return pl.pallas_call(
        write_out,
        out_shape=tuple(jax.ShapeDtypeStruct(shape, bf16) for shape in shapes),
        in_specs=[pl.BlockSpec(memory_space=pltpu.VMEM)] * 3,
        out_specs=[pl.BlockSpec(memory_space=pltpu.HBM)] * 3,
        scratch_shapes=[dma((3,))],
    )(*[pltpu.with_memory_space_constraint(r, pltpu.VMEM) for r in results])


def solution(mesh):
    in_specs = (
        P(("grp", "ep"), None),
        P(),
        P(None, "tp"),
        P(None, "tp"),
        P(None, "tp"),
        P(("grp", "ep"), "tp", None),
        P(("grp", "ep"), "tp", None),
        P(("grp", "ep")),
        P("tp"),
        P(None, "tp"),
        P(),
        P(("grp", "ep"), None),
        P(("grp", "ep"), None),
        P("ep", None, "tp"),
        P("ep", None, "tp"),
        P("ep", "tp", None),
    )
    out_specs = (P(("grp", "ep"), "tp"), P(("grp", "ep"), "tp"), P(("grp", "ep"), "tp"))
    body = functools.partial(shards, mesh.shape["tp"], mesh.shape["ep"])
    return jax.shard_map(body, mesh=mesh, in_specs=in_specs, out_specs=out_specs, check_vma=False)
```

```python
import functools

import jax
import jax.numpy as jnp
from jax import lax
from jax.experimental import pallas as pl
from jax.experimental.pallas import tpu as pltpu
from jax.sharding import PartitionSpec as P

HEAD_SIZE = 64
LANES = 128
CORES = 2
epsilon = 1e-06
f32 = jnp.float32
bf16 = jnp.bfloat16


def iota(shape, dim):
    return lax.broadcasted_iota(jnp.int32, shape, dim)


def hops(step, count):
    return min(step % count, -step % count)


def far_first(count):
    return sorted(range(1, count), key=lambda step: -hops(step, count))


def near_first(count):
    return sorted(range(1, count), key=lambda step: hops(step, count))


def nt_dot(left, right):
    return lax.dot_general(left, right, (((1,), (1,)), ((), ())), preferred_element_type=f32)


def kernel(
    n_tp,
    n_ep,
    tok_hbm,
    again_hbm,
    wq_hbm,
    wk_hbm,
    wv_hbm,
    key_hbm,
    val_hbm,
    len_hbm,
    bias_hbm,
    wo_hbm,
    fgain_hbm,
    ids_hbm,
    rw_hbm,
    wg_hbm,
    wu_hbm,
    wd_hbm,
    mixed_ref,
    nk_ref,
    nv_ref,
    tok,
    again,
    wq,
    wk,
    wv,
    key,
    val,
    lens,
    bias,
    wo,
    fgain,
    ids,
    rw,
    wg,
    wu,
    wd,
    rows_pad,
    idp,
    rwp,
    tri,
    place,
    combine,
    hid,
    hg,
    zsend,
    zrecv,
    xg,
    rsend,
    rrecv,
    ysend,
    ret,
    local_sem,
    h_ssem,
    h_rsem,
    z_ssem,
    z_rsem,
    g_ssem,
    g_rsem,
    r_ssem,
    r_rsem,
    y_ssem,
    y_rsem,
):
    tp = lax.axis_index("tp")
    ep = lax.axis_index("ep")
    core = lax.rem(ep, CORES)
    chip = ep // CORES
    chips = n_ep // CORES
    half = n_ep // 2
    seq_rows = tok.shape[0]
    slots = 2 * n_ep

    def copies_of(first, pairs):
        made = [
            pltpu.make_async_copy(source, target, local_sem.at[first + number])
            for number, (source, target) in enumerate(pairs)
        ]
        for copy in made:
            copy.start()
        return made

    c_tok, c_again, c_wq, c_len, c_bias, c_key, c_val = copies_of(
        0,
        (
            (tok_hbm, tok),
            (again_hbm, again),
            (wq_hbm, wq),
            (len_hbm, lens),
            (bias_hbm, bias),
            (key_hbm, key),
            (val_hbm, val),
        ),
    )

    def wrap(number, count):
        return jnp.where(number >= count, number - count, number)

    barrier = pltpu.get_barrier_semaphore()
    for step in far_first(n_tp):
        pl.semaphore_signal(barrier, inc=1, device_id={"tp": wrap(tp + step, n_tp)})

    @pl.loop(1, n_ep)
    def _(step):
        pl.semaphore_signal(barrier, inc=1, device_id={"ep": wrap(ep + step, n_ep)})

    def landed(view, sem):
        pltpu.make_async_copy(view, view, sem).wait()

    tri_len = tri.shape[0]
    tri[...] = (iota((tri_len, tri_len), 0) > iota((tri_len, tri_len), 1)).astype(f32).astype(bf16)
    rows_pad[...] = jnp.zeros_like(rows_pad)
    hid[...] = jnp.zeros_like(hid)
    idp[...] = jnp.full(idp.shape, -1.0, f32)
    rwp[...] = jnp.zeros_like(rwp)

    c_tok.wait()
    c_again.wait()
    token_rows = tok[...].astype(f32)
    mean_sq = jnp.mean(token_rows * token_rows, axis=1, keepdims=True)
    normed = (token_rows * lax.rsqrt(mean_sq + epsilon) * again[...]).astype(bf16)
    c_wq.wait()
    queries = jnp.dot(normed, wq[...], preferred_element_type=f32).astype(bf16).astype(f32)
    rows_pad[pl.ds(0, seq_rows), :] = queries * HEAD_SIZE ** (-0.5)
    padded = rows_pad[...]
    pad_rows = padded.shape[0]
    low = iota(padded.shape, 1) < HEAD_SIZE
    turned = pltpu.roll(padded, HEAD_SIZE, axis=1)
    both = jnp.concatenate([jnp.where(low, padded, turned), jnp.where(low, turned, padded)], axis=0)
    cols = key.shape[0]
    wide = jnp.concatenate([both] * (cols // LANES), axis=1)
    own_block = (iota(wide.shape, 1) // HEAD_SIZE) == lax.rem(iota(wide.shape, 0), pad_rows)
    spread = jnp.where(own_block, wide, 0.0).astype(bf16)

    c_len.wait()
    c_bias.wait()
    idp[pl.ds(2, 1), pl.ds(0, seq_rows)] = lens[...].astype(f32)
    len_row = jnp.broadcast_to(idp[pl.ds(2, 1), :], (2 * pad_rows, LANES))
    own_lane = iota(len_row.shape, 1) == lax.rem(iota(len_row.shape, 0), pad_rows)
    len_col = jnp.sum(jnp.where(own_lane, len_row, 0.0), axis=1, keepdims=True)
    bias_col = jnp.where(
        iota((2 * pad_rows, 1), 0) < pad_rows, bias[pl.ds(0, 1), pl.ds(0, 1)], bias[pl.ds(0, 1), pl.ds(1, 1)]
    )

    c_key.wait()
    c_wo, c_wk, c_wv, c_ids, c_rw, c_fgain = copies_of(
        7, ((wo_hbm, wo), (wk_hbm, wk), (wv_hbm, wv), (ids_hbm, ids), (rw_hbm, rw), (fgain_hbm, fgain))
    )
    scores = jnp.dot(spread, key[...], preferred_element_type=f32) + bias_col
    in_cache = iota(scores.shape, 1).astype(f32) < len_col
    log_rest = -(jnp.maximum(scores, 0.0) + jnp.log1p(jnp.exp(-jnp.abs(scores))))
    log_rest = jnp.where(in_cache, log_rest, 0.0)
    cache_len = scores.shape[1]
    chunk_count = cache_len // tri_len
    high = log_rest.astype(bf16)
    rest = (log_rest - high.astype(f32)).astype(bf16)
    stacked = jnp.concatenate(
        [part[:, c * tri_len : (c + 1) * tri_len] for part in (high, rest) for c in range(chunk_count)], axis=0
    )
    within = jnp.dot(stacked, tri[...], preferred_element_type=f32)
    tails = []
    carry = jnp.zeros((2 * pad_rows, 1), f32)
    span = 2 * pad_rows
    for c in reversed(range(chunk_count)):
        inner = within[c * span : (c + 1) * span] + within[(chunk_count + c) * span : (chunk_count + c + 1) * span]
        tails.append(inner + carry)
        carry = carry + inner[:, 0:1] + log_rest[:, c * tri_len : c * tri_len + 1]
    tail = jnp.concatenate(tails[::-1], axis=1)
    breaks = jnp.where(in_cache, jnp.exp(scores + log_rest + tail), 0.0).astype(bf16)
    c_val.wait()
    mixed_values = nt_dot(breaks, val[...])
    mixed_values = jnp.where(own_block, mixed_values, 0.0)
    folded = mixed_values[:, 0:LANES]
    for c in range(1, cols // LANES):
        folded = folded + mixed_values[:, c * LANES : (c + 1) * LANES]
    folded = folded + pltpu.roll(folded, HEAD_SIZE, axis=1)
    heads = jnp.where(low, folded[:pad_rows], folded[pad_rows:]).astype(bf16)
    hg[tp] = heads

    pl.semaphore_wait(barrier, (n_tp - 1) + (n_ep - 1))
    for step in far_first(n_tp):
        pltpu.make_async_remote_copy(
            hg.at[tp], hg.at[tp], h_ssem, h_rsem, device_id={"tp": wrap(tp + step, n_tp)}
        ).start()

    c_wg, c_wu, c_wd = copies_of(0, ((wg_hbm, wg), (wu_hbm, wu), (wd_hbm, wd)))
    c_wk.wait()
    c_wv.wait()
    nk_ref[...] = nt_dot(normed, wk[...]).astype(bf16)
    nv_ref[...] = nt_dot(normed, wv[...]).astype(bf16)
    c_ids.wait()
    c_rw.wait()
    top_count = ids.shape[0]
    idp[pl.ds(0, top_count), pl.ds(0, seq_rows)] = ids[...].astype(f32)
    rwp[pl.ds(0, top_count), pl.ds(0, seq_rows)] = rw[...]
    slot_expert = (iota((slots, LANES), 0) // 2).astype(f32)
    slot_rank = lax.rem(iota((slots, LANES), 0), 2).astype(f32)
    hits = [(slot_expert == idp[pl.ds(k, 1), :]).astype(f32) for k in range(top_count)]
    any_hit = sum(hits)
    upper = (iota((LANES, LANES), 0) < iota((LANES, LANES), 1)).astype(f32).astype(bf16)
    before = jnp.dot(any_hit.astype(bf16), upper, preferred_element_type=f32)
    taken = jnp.where(before == slot_rank, 1.0, 0.0)
    place[...] = (any_hit * taken).astype(bf16)
    weighted = sum(hits[k] * rwp[pl.ds(k, 1), :] for k in range(top_count)) * taken
    weighted_t = weighted.T[: combine.shape[0] // 2]
    weighted_high = weighted_t.astype(bf16)
    combine[pl.ds(0, pad_rows), :] = weighted_high
    combine[pl.ds(pad_rows, pad_rows), :] = (weighted_t - weighted_high.astype(f32)).astype(bf16)
    c_fgain.wait()
    own_cols = pl.ds(pl.multiple_of(tp * LANES, LANES), LANES)
    own_tokens = tok[:, own_cols].astype(f32)
    own_gain = fgain[:, own_cols]

    c_wo.wait()
    inverse_sq = 1.0 / (fgain[...] * fgain[...])
    peers = pl.ds(0, n_tp - 1)
    landed(hg.at[peers], h_rsem)
    all_heads = jnp.concatenate([hg[peer] for peer in range(n_tp)], axis=1)
    attn_out = jnp.dot(all_heads, wo[...], preferred_element_type=f32)
    hid[pl.ds(0, seq_rows), :] = own_tokens + attn_out[:seq_rows]
    scaled = (hid[...] * own_gain).astype(bf16)
    outgoing = jnp.dot(place[...], scaled, preferred_element_type=f32).astype(bf16)
    zsend[...] = outgoing.reshape(zsend.shape)

    own_part = ep // half
    for step in far_first(chips):
        to_chip = wrap(chip + step, chips)
        for to_core in range(CORES):
            to_ep = to_chip * CORES + to_core
            pltpu.make_async_remote_copy(
                zsend.at[to_ep], zrecv.at[ep], z_ssem, z_rsem.at[own_part], device_id={"ep": to_ep}
            ).start()
    partner = chip * CORES + (1 - core)
    pltpu.make_async_remote_copy(
        zsend.at[partner], zrecv.at[ep], z_ssem, z_rsem.at[own_part], device_id={"ep": partner}
    ).start()
    pltpu.make_async_copy(zsend.at[ep], zrecv.at[ep], z_rsem.at[own_part]).start()

    c_wg.wait()
    c_wu.wait()
    c_wd.wait()
    for part in range(2):
        span_at = pl.ds(part * half, half)
        landed(zrecv.at[span_at], z_rsem.at[part])
        xg[part, tp] = zrecv[span_at].reshape(slots // 2, LANES)
        for step in far_first(n_tp):
            pltpu.make_async_remote_copy(
                xg.at[part, tp],
                xg.at[part, tp],
                g_ssem.at[part],
                g_rsem.at[part],
                device_id={"tp": wrap(tp + step, n_tp)},
            ).start()
        landed(xg.at[part, peers], g_rsem.at[part])
        rows = jnp.concatenate([xg[part, peer] for peer in range(n_tp)], axis=1)
        gate = jnp.dot(rows, wg[...], preferred_element_type=f32)
        up = jnp.dot(rows, wu[...], preferred_element_type=f32)
        plain = rows.astype(f32)
        sum_sq = jnp.sum(plain * plain * inverse_sq, axis=1, keepdims=True)
        scale = lax.rsqrt(sum_sq / (n_tp * LANES) + epsilon)
        gate = gate * scale
        up = up * scale
        hidden_act = (gate / (1.0 + jnp.exp(-gate)) * up).astype(bf16)
        partial_value = jnp.dot(hidden_act, wd[...], preferred_element_type=f32).astype(bf16)
        for c in range(n_tp):
            rsend[part, c] = partial_value[:, c * LANES : (c + 1) * LANES]
        for step in far_first(n_tp):
            peer = wrap(tp + step, n_tp)
            pltpu.make_async_remote_copy(
                rsend.at[part, peer], rrecv.at[part, tp], r_ssem.at[part], r_rsem.at[part], device_id={"tp": peer}
            ).start()
        rrecv[part, tp] = rsend[part, tp]
        landed(rrecv.at[part, peers], r_rsem.at[part])
        total = rrecv[part, 0].astype(f32)
        for peer in range(1, n_tp):
            total += rrecv[part, peer].astype(f32)
        ysend[span_at] = total.astype(bf16).reshape(half, 2, LANES)
        for to_ep in range(half * part, half * (part + 1)):

            @pl.when(to_ep != ep)
            def _():
                pltpu.make_async_remote_copy(
                    ysend.at[to_ep], ret.at[ep], y_ssem, y_rsem, device_id={"ep": to_ep}
                ).start()

    pltpu.make_async_copy(ysend.at[ep], ret.at[ep], y_rsem).start()
    landed(hg.at[peers], h_ssem)
    landed(zsend.at[pl.ds(0, n_ep - 1)], z_ssem)
    for part in range(2):
        landed(xg.at[part, peers], g_ssem.at[part])
        landed(rsend.at[part, peers], r_ssem.at[part])
    landed(ysend.at[pl.ds(0, n_ep - 1)], y_ssem)
    landed(ret, y_rsem)
    picked = jnp.dot(combine[...], ret[...].reshape(slots, LANES), preferred_element_type=f32)
    routed_sum = picked[:pad_rows] + picked[pad_rows:]
    mixed_ref[...] = (hid[pl.ds(0, seq_rows), :] + routed_sum[:seq_rows]).astype(bf16)


def write_out(*refs):
    count = len(refs) // 2
    copies = [pltpu.make_async_copy(refs[n], refs[count + n], refs[-1].at[n]) for n in range(count)]
    for copy in copies:
        copy.start()
    for copy in copies:
        copy.wait()


def shards(
    n_tp,
    n_ep,
    tokens,
    attn_gain,
    w_query,
    w_key,
    w_value,
    key_cache,
    value_cache,
    lengths,
    head_bias,
    w_out,
    ffn_gain,
    route_ids,
    route_weights,
    w_gate,
    w_up,
    w_down,
):
    seq_rows, model_width = tokens.shape
    cache_len = key_cache.shape[2]
    kv_cols = key_cache.shape[1]
    pad_rows = 16
    slots = 2 * n_ep
    operands = (
        tokens,
        attn_gain.reshape(1, model_width),
        w_query,
        w_key.T,
        w_value.T,
        key_cache.reshape(seq_rows * kv_cols, cache_len),
        value_cache.reshape(seq_rows * kv_cols, cache_len),
        lengths.reshape(1, seq_rows),
        head_bias.reshape(1, head_bias.shape[0]),
        w_out,
        ffn_gain.reshape(1, model_width),
        route_ids.T,
        route_weights.T,
        w_gate[0],
        w_up[0],
        w_down[0],
    )
    dma = pltpu.SemaphoreType.DMA
    scratch = [pltpu.VMEM(op.shape, op.dtype) for op in operands] + [
        pltpu.VMEM((pad_rows, LANES), f32),
        pltpu.VMEM((8, LANES), f32),
        pltpu.VMEM((8, LANES), f32),
        pltpu.VMEM((256, 256), bf16),
        pltpu.VMEM((slots, LANES), bf16),
        pltpu.VMEM((2 * pad_rows, slots), bf16),
        pltpu.VMEM((LANES, LANES), f32),
        pltpu.VMEM((n_tp, pad_rows, LANES), bf16),
        pltpu.VMEM((n_ep, 2, LANES), bf16),
        pltpu.VMEM((n_ep, 2, LANES), bf16),
        pltpu.VMEM((2, n_tp, slots // 2, LANES), bf16),
        pltpu.VMEM((2, n_tp, slots // 2, LANES), bf16),
        pltpu.VMEM((2, n_tp, slots // 2, LANES), bf16),
        pltpu.VMEM((n_ep, 2, LANES), bf16),
        pltpu.VMEM((n_ep, 2, LANES), bf16),
        dma((13,)),
        dma,
        dma,
        dma,
        dma((2,)),
        dma((2,)),
        dma((2,)),
        dma((2,)),
        dma((2,)),
        dma,
        dma,
    ]
    shapes = (
        (seq_rows, w_out.shape[1]),
        (seq_rows, w_key.shape[1]),
        (seq_rows, w_value.shape[1]),
    )
    results = pl.pallas_call(
        functools.partial(kernel, n_tp, n_ep),
        out_shape=tuple(pltpu.VMEM(shape, bf16) for shape in shapes),
        in_specs=[pl.BlockSpec(memory_space=pltpu.HBM)] * len(operands),
        out_specs=[pl.BlockSpec(memory_space=pltpu.VMEM)] * 3,
        scratch_shapes=scratch,
        compiler_params=pltpu.CompilerParams(collective_id=0, has_side_effects=True),
    )(*operands)
    return pl.pallas_call(
        write_out,
        out_shape=tuple(jax.ShapeDtypeStruct(shape, bf16) for shape in shapes),
        in_specs=[pl.BlockSpec(memory_space=pltpu.VMEM)] * 3,
        out_specs=[pl.BlockSpec(memory_space=pltpu.HBM)] * 3,
        scratch_shapes=[dma((3,))],
    )(*[pltpu.with_memory_space_constraint(r, pltpu.VMEM) for r in results])


def solution(mesh):
    in_specs = (
        P(("grp", "ep"), None),
        P(),
        P(None, "tp"),
        P(None, "tp"),
        P(None, "tp"),
        P(("grp", "ep"), "tp", None),
        P(("grp", "ep"), "tp", None),
        P(("grp", "ep")),
        P("tp"),
        P(None, "tp"),
        P(),
        P(("grp", "ep"), None),
        P(("grp", "ep"), None),
        P("ep", None, "tp"),
        P("ep", None, "tp"),
        P("ep", "tp", None),
    )
    out_specs = (P(("grp", "ep"), "tp"), P(("grp", "ep"), "tp"), P(("grp", "ep"), "tp"))
    body = functools.partial(shards, mesh.shape["tp"], mesh.shape["ep"])
    return jax.shard_map(body, mesh=mesh, in_specs=in_specs, out_specs=out_specs, check_vma=False)
```

```python
import functools

import jax
import jax.numpy as jnp
from jax import lax
from jax.experimental import pallas as pl
from jax.experimental.pallas import tpu as pltpu
from jax.sharding import PartitionSpec as P

HEAD_SIZE = 64
LANES = 128
CORES = 2
epsilon = 1e-06
f32 = jnp.float32
bf16 = jnp.bfloat16


def iota(shape, dim):
    return lax.broadcasted_iota(jnp.int32, shape, dim)


def hops(step, count):
    return min(step % count, -step % count)


def far_first(count):
    return sorted(range(1, count), key=lambda step: -hops(step, count))


def near_first(count):
    return sorted(range(1, count), key=lambda step: hops(step, count))


def nt_dot(left, right):
    return lax.dot_general(left, right, (((1,), (1,)), ((), ())), preferred_element_type=f32)


def kernel(
    n_tp,
    n_ep,
    tok_hbm,
    again_hbm,
    wq_hbm,
    wk_hbm,
    wv_hbm,
    key_hbm,
    val_hbm,
    len_hbm,
    bias_hbm,
    wo_hbm,
    fgain_hbm,
    ids_hbm,
    rw_hbm,
    wg_hbm,
    wu_hbm,
    wd_hbm,
    mixed_ref,
    nk_ref,
    nv_ref,
    tok,
    again,
    wq,
    wk,
    wv,
    key,
    val,
    lens,
    bias,
    wo,
    fgain,
    ids,
    rw,
    wg,
    wu,
    wd,
    rows_pad,
    idp,
    rwp,
    tri,
    place,
    combine,
    hid,
    hg,
    zsend,
    zrecv,
    xg,
    rsend,
    rrecv,
    ysend,
    ret,
    local_sem,
    h_ssem,
    h_rsem,
    z_ssem,
    z_rsem,
    g_ssem,
    g_rsem,
    r_ssem,
    r_rsem,
    y_ssem,
    y_rsem,
    ready,
):
    tp = lax.axis_index("tp")
    ep = lax.axis_index("ep")
    core = lax.rem(ep, CORES)
    chip = ep // CORES
    chips = n_ep // CORES
    seq_rows = tok.shape[0]
    slots = 2 * n_ep

    def copies_of(first, pairs):
        made = [
            pltpu.make_async_copy(source, target, local_sem.at[first + number])
            for number, (source, target) in enumerate(pairs)
        ]
        for copy in made:
            copy.start()
        return made

    c_tok, c_again, c_wq, c_len, c_bias, c_key, c_val = copies_of(
        0,
        (
            (tok_hbm, tok),
            (again_hbm, again),
            (wq_hbm, wq),
            (len_hbm, lens),
            (bias_hbm, bias),
            (key_hbm, key),
            (val_hbm, val),
        ),
    )

    def wrap(number, count):
        return jnp.where(number >= count, number - count, number)

    barrier = pltpu.get_barrier_semaphore()
    column = tp == 0
    topmost = jnp.logical_and(column, ep == 0)
    partner = chip * CORES + (1 - core)
    for step in far_first(n_tp):
        pl.semaphore_signal(barrier, inc=1, device_id={"tp": wrap(tp + step, n_tp)})

    @pl.loop(jnp.where(topmost, n_ep, ep + 1), n_ep)
    def _(above):
        pl.semaphore_signal(barrier, inc=1, device_id={"ep": above})

    @pl.when(jnp.logical_and(column, ep > 0))
    def _():
        pl.semaphore_signal(barrier, inc=1, device_id={"ep": 0})

    def landed(view, sem):
        pltpu.make_async_copy(view, view, sem).wait()

    tri_len = tri.shape[0]
    tri[...] = (iota((tri_len, tri_len), 0) > iota((tri_len, tri_len), 1)).astype(f32).astype(bf16)
    rows_pad[...] = jnp.zeros_like(rows_pad)
    hid[...] = jnp.zeros_like(hid)
    idp[...] = jnp.full(idp.shape, -1.0, f32)
    rwp[...] = jnp.zeros_like(rwp)

    c_tok.wait()
    c_again.wait()
    token_rows = tok[...].astype(f32)
    mean_sq = jnp.mean(token_rows * token_rows, axis=1, keepdims=True)
    normed = (token_rows * lax.rsqrt(mean_sq + epsilon) * again[...]).astype(bf16)
    c_wq.wait()
    queries = jnp.dot(normed, wq[...], preferred_element_type=f32).astype(bf16).astype(f32)
    rows_pad[pl.ds(0, seq_rows), :] = queries * HEAD_SIZE ** (-0.5)
    padded = rows_pad[...]
    pad_rows = padded.shape[0]
    low = iota(padded.shape, 1) < HEAD_SIZE
    turned = pltpu.roll(padded, HEAD_SIZE, axis=1)
    both = jnp.concatenate([jnp.where(low, padded, turned), jnp.where(low, turned, padded)], axis=0)
    cols = key.shape[0]
    wide = jnp.concatenate([both] * (cols // LANES), axis=1)
    own_block = (iota(wide.shape, 1) // HEAD_SIZE) == lax.rem(iota(wide.shape, 0), pad_rows)
    spread = jnp.where(own_block, wide, 0.0).astype(bf16)

    c_len.wait()
    c_bias.wait()
    idp[pl.ds(2, 1), pl.ds(0, seq_rows)] = lens[...].astype(f32)
    len_row = jnp.broadcast_to(idp[pl.ds(2, 1), :], (2 * pad_rows, LANES))
    own_lane = iota(len_row.shape, 1) == lax.rem(iota(len_row.shape, 0), pad_rows)
    len_col = jnp.sum(jnp.where(own_lane, len_row, 0.0), axis=1, keepdims=True)
    bias_col = jnp.where(
        iota((2 * pad_rows, 1), 0) < pad_rows, bias[pl.ds(0, 1), pl.ds(0, 1)], bias[pl.ds(0, 1), pl.ds(1, 1)]
    )

    c_key.wait()
    c_wo, c_wk, c_wv, c_ids, c_rw, c_fgain = copies_of(
        7, ((wo_hbm, wo), (wk_hbm, wk), (wv_hbm, wv), (ids_hbm, ids), (rw_hbm, rw), (fgain_hbm, fgain))
    )
    scores = jnp.dot(spread, key[...], preferred_element_type=f32) + bias_col
    in_cache = iota(scores.shape, 1).astype(f32) < len_col
    log_rest = -(jnp.maximum(scores, 0.0) + jnp.log1p(jnp.exp(-jnp.abs(scores))))
    log_rest = jnp.where(in_cache, log_rest, 0.0)
    cache_len = scores.shape[1]
    chunk_count = cache_len // tri_len
    high = log_rest.astype(bf16)
    rest = (log_rest - high.astype(f32)).astype(bf16)
    stacked = jnp.concatenate(
        [part[:, c * tri_len : (c + 1) * tri_len] for part in (high, rest) for c in range(chunk_count)], axis=0
    )
    within = jnp.dot(stacked, tri[...], preferred_element_type=f32)
    tails = []
    carry = jnp.zeros((2 * pad_rows, 1), f32)
    span = 2 * pad_rows
    for c in reversed(range(chunk_count)):
        inner = within[c * span : (c + 1) * span] + within[(chunk_count + c) * span : (chunk_count + c + 1) * span]
        tails.append(inner + carry)
        carry = carry + inner[:, 0:1] + log_rest[:, c * tri_len : c * tri_len + 1]
    tail = jnp.concatenate(tails[::-1], axis=1)
    breaks = jnp.where(in_cache, jnp.exp(scores + log_rest + tail), 0.0).astype(bf16)
    c_val.wait()
    mixed_values = nt_dot(breaks, val[...])
    mixed_values = jnp.where(own_block, mixed_values, 0.0)
    folded = mixed_values[:, 0:LANES]
    for c in range(1, cols // LANES):
        folded = folded + mixed_values[:, c * LANES : (c + 1) * LANES]
    folded = folded + pltpu.roll(folded, HEAD_SIZE, axis=1)
    heads = jnp.where(low, folded[:pad_rows], folded[pad_rows:]).astype(bf16)
    hg[tp] = heads

    lowest = jnp.where(column, 1, 0)
    pl.semaphore_wait(barrier, (n_tp - 1) + jnp.where(topmost, n_ep - 1, ep - lowest))
    for step in far_first(n_tp):
        pltpu.make_async_remote_copy(
            hg.at[tp], hg.at[tp], h_ssem, h_rsem, device_id={"tp": wrap(tp + step, n_tp)}
        ).start()

    @pl.loop(lowest, jnp.where(topmost, n_ep, ep))
    def _(below):
        pl.semaphore_signal(ready.at[chip], inc=1, device_id={"ep": below})

    c_wg, c_wu, c_wd = copies_of(0, ((wg_hbm, wg), (wu_hbm, wu), (wd_hbm, wd)))
    c_wk.wait()
    c_wv.wait()
    nk_ref[...] = nt_dot(normed, wk[...]).astype(bf16)
    nv_ref[...] = nt_dot(normed, wv[...]).astype(bf16)
    c_ids.wait()
    c_rw.wait()
    top_count = ids.shape[0]
    idp[pl.ds(0, top_count), pl.ds(0, seq_rows)] = ids[...].astype(f32)
    rwp[pl.ds(0, top_count), pl.ds(0, seq_rows)] = rw[...]
    slot_expert = (iota((slots, LANES), 0) // 2).astype(f32)
    slot_rank = lax.rem(iota((slots, LANES), 0), 2).astype(f32)
    hits = [(slot_expert == idp[pl.ds(k, 1), :]).astype(f32) for k in range(top_count)]
    any_hit = sum(hits)
    upper = (iota((LANES, LANES), 0) < iota((LANES, LANES), 1)).astype(f32).astype(bf16)
    before = jnp.dot(any_hit.astype(bf16), upper, preferred_element_type=f32)
    taken = jnp.where(before == slot_rank, 1.0, 0.0)
    place[...] = (any_hit * taken).astype(bf16)
    weighted = sum(hits[k] * rwp[pl.ds(k, 1), :] for k in range(top_count)) * taken
    weighted_t = weighted.T[: combine.shape[0] // 2]
    weighted_high = weighted_t.astype(bf16)
    combine[pl.ds(0, pad_rows), :] = weighted_high
    combine[pl.ds(pad_rows, pad_rows), :] = (weighted_t - weighted_high.astype(f32)).astype(bf16)
    c_fgain.wait()
    own_cols = pl.ds(pl.multiple_of(tp * LANES, LANES), LANES)
    own_tokens = tok[:, own_cols].astype(f32)
    own_gain = fgain[:, own_cols]

    c_wo.wait()
    inverse_sq = 1.0 / (fgain[...] * fgain[...])
    peers = pl.ds(0, n_tp - 1)
    landed(hg.at[peers], h_rsem)
    all_heads = jnp.concatenate([hg[peer] for peer in range(n_tp)], axis=1)
    attn_out = jnp.dot(all_heads, wo[...], preferred_element_type=f32)
    hid[pl.ds(0, seq_rows), :] = own_tokens + attn_out[:seq_rows]
    scaled = (hid[...] * own_gain).astype(bf16)
    outgoing = jnp.dot(place[...], scaled, preferred_element_type=f32).astype(bf16)
    zsend[...] = outgoing.reshape(zsend.shape)

    bounds = (0, n_ep // 4, n_ep)
    own_group = jnp.where(ep >= bounds[1], 1, 0)
    def send_slots(to_ep):
        @pl.when(to_ep != ep)
        def _():
            pltpu.make_async_remote_copy(
                zsend.at[to_ep], zrecv.at[ep], z_ssem, z_rsem.at[own_group], device_id={"ep": to_ep}
            ).start()

    for to_chip in range(chips):

        @pl.when(jnp.logical_and(to_chip > chip, jnp.logical_not(topmost)))
        def _():
            pl.semaphore_wait(ready.at[to_chip], CORES)

        @pl.when(jnp.logical_and(jnp.logical_and(to_chip == chip, core == 0), jnp.logical_not(topmost)))
        def _():
            pl.semaphore_wait(ready.at[to_chip], 1)

        for to_ep in range(max(1, to_chip * CORES), (to_chip + 1) * CORES):
            send_slots(to_ep)

    @pl.when(jnp.logical_and(column, ep > 0))
    def _():
        pl.semaphore_wait(ready.at[0], 1)

    send_slots(0)
    pltpu.make_async_copy(zsend.at[ep], zrecv.at[ep], z_rsem.at[own_group]).start()

    c_wg.wait()
    c_wu.wait()
    c_wd.wait()
    for group, (first, last) in enumerate(zip(bounds[:-1], bounds[1:])):
        count = last - first
        eps = pl.ds(first, count)
        here = pl.ds(2 * first, 2 * count)
        landed(zrecv.at[eps], z_rsem.at[group])
        xg[tp, here] = zrecv[eps].reshape(2 * count, LANES)
        for step in far_first(n_tp):
            pltpu.make_async_remote_copy(
                xg.at[tp, here],
                xg.at[tp, here],
                g_ssem.at[group],
                g_rsem.at[group],
                device_id={"tp": wrap(tp + step, n_tp)},
            ).start()
        landed(xg.at[peers, here], g_rsem.at[group])
        rows = jnp.concatenate([xg[peer, here] for peer in range(n_tp)], axis=1)
        gate = jnp.dot(rows, wg[...], preferred_element_type=f32)
        up = jnp.dot(rows, wu[...], preferred_element_type=f32)
        plain = rows.astype(f32)
        sum_sq = jnp.sum(plain * plain * inverse_sq, axis=1, keepdims=True)
        scale = lax.rsqrt(sum_sq / (n_tp * LANES) + epsilon)
        gate = gate * scale
        up = up * scale
        hidden_act = (gate / (1.0 + jnp.exp(-gate)) * up).astype(bf16)
        partial_value = jnp.dot(hidden_act, wd[...], preferred_element_type=f32).astype(bf16)
        for c in range(n_tp):
            rsend[c, here] = partial_value[:, c * LANES : (c + 1) * LANES]
        for step in far_first(n_tp):
            peer = wrap(tp + step, n_tp)
            pltpu.make_async_remote_copy(
                rsend.at[peer, here], rrecv.at[tp, here], r_ssem.at[group], r_rsem.at[group], device_id={"tp": peer}
            ).start()
        rrecv[tp, here] = rsend[tp, here]
        landed(rrecv.at[peers, here], r_rsem.at[group])
        total = rrecv[0, here].astype(f32)
        for peer in range(1, n_tp):
            total += rrecv[peer, here].astype(f32)
        ysend[eps] = total.astype(bf16).reshape(count, 2, LANES)
        for to_ep in range(first, last):

            @pl.when(to_ep != ep)
            def _():
                pltpu.make_async_remote_copy(
                    ysend.at[to_ep], ret.at[ep], y_ssem, y_rsem, device_id={"ep": to_ep}
                ).start()

    pltpu.make_async_copy(ysend.at[ep], ret.at[ep], y_rsem).start()
    landed(hg.at[peers], h_ssem)
    landed(zsend.at[pl.ds(0, n_ep - 1)], z_ssem)
    for group, (first, last) in enumerate(zip(bounds[:-1], bounds[1:])):
        here = pl.ds(2 * first, 2 * (last - first))
        landed(xg.at[peers, here], g_ssem.at[group])
        landed(rsend.at[peers, here], r_ssem.at[group])
    landed(ysend.at[pl.ds(0, n_ep - 1)], y_ssem)
    landed(ret, y_rsem)
    picked = jnp.dot(combine[...], ret[...].reshape(slots, LANES), preferred_element_type=f32)
    routed_sum = picked[:pad_rows] + picked[pad_rows:]
    mixed_ref[...] = (hid[pl.ds(0, seq_rows), :] + routed_sum[:seq_rows]).astype(bf16)


def write_out(*refs):
    count = len(refs) // 2
    copies = [pltpu.make_async_copy(refs[n], refs[count + n], refs[-1].at[n]) for n in range(count)]
    for copy in copies:
        copy.start()
    for copy in copies:
        copy.wait()


def shards(
    n_tp,
    n_ep,
    tokens,
    attn_gain,
    w_query,
    w_key,
    w_value,
    key_cache,
    value_cache,
    lengths,
    head_bias,
    w_out,
    ffn_gain,
    route_ids,
    route_weights,
    w_gate,
    w_up,
    w_down,
):
    seq_rows, model_width = tokens.shape
    cache_len = key_cache.shape[2]
    kv_cols = key_cache.shape[1]
    pad_rows = 16
    slots = 2 * n_ep
    operands = (
        tokens,
        attn_gain.reshape(1, model_width),
        w_query,
        w_key.T,
        w_value.T,
        key_cache.reshape(seq_rows * kv_cols, cache_len),
        value_cache.reshape(seq_rows * kv_cols, cache_len),
        lengths.reshape(1, seq_rows),
        head_bias.reshape(1, head_bias.shape[0]),
        w_out,
        ffn_gain.reshape(1, model_width),
        route_ids.T,
        route_weights.T,
        w_gate[0],
        w_up[0],
        w_down[0],
    )
    dma = pltpu.SemaphoreType.DMA
    scratch = [pltpu.VMEM(op.shape, op.dtype) for op in operands] + [
        pltpu.VMEM((pad_rows, LANES), f32),
        pltpu.VMEM((8, LANES), f32),
        pltpu.VMEM((8, LANES), f32),
        pltpu.VMEM((256, 256), bf16),
        pltpu.VMEM((slots, LANES), bf16),
        pltpu.VMEM((2 * pad_rows, slots), bf16),
        pltpu.VMEM((LANES, LANES), f32),
        pltpu.VMEM((n_tp, pad_rows, LANES), bf16),
        pltpu.VMEM((n_ep, 2, LANES), bf16),
        pltpu.VMEM((n_ep, 2, LANES), bf16),
        pltpu.VMEM((n_tp, slots, LANES), bf16),
        pltpu.VMEM((n_tp, slots, LANES), bf16),
        pltpu.VMEM((n_tp, slots, LANES), bf16),
        pltpu.VMEM((n_ep, 2, LANES), bf16),
        pltpu.VMEM((n_ep, 2, LANES), bf16),
        dma((13,)),
        dma,
        dma,
        dma,
        dma((2,)),
        dma((2,)),
        dma((2,)),
        dma((2,)),
        dma((2,)),
        dma,
        dma,
        pltpu.SemaphoreType.REGULAR((n_ep // CORES,)),
    ]
    shapes = (
        (seq_rows, w_out.shape[1]),
        (seq_rows, w_key.shape[1]),
        (seq_rows, w_value.shape[1]),
    )
    results = pl.pallas_call(
        functools.partial(kernel, n_tp, n_ep),
        out_shape=tuple(pltpu.VMEM(shape, bf16) for shape in shapes),
        in_specs=[pl.BlockSpec(memory_space=pltpu.HBM)] * len(operands),
        out_specs=[pl.BlockSpec(memory_space=pltpu.VMEM)] * 3,
        scratch_shapes=scratch,
        compiler_params=pltpu.CompilerParams(collective_id=0, has_side_effects=True),
    )(*operands)
    return pl.pallas_call(
        write_out,
        out_shape=tuple(jax.ShapeDtypeStruct(shape, bf16) for shape in shapes),
        in_specs=[pl.BlockSpec(memory_space=pltpu.VMEM)] * 3,
        out_specs=[pl.BlockSpec(memory_space=pltpu.HBM)] * 3,
        scratch_shapes=[dma((3,))],
    )(*[pltpu.with_memory_space_constraint(r, pltpu.VMEM) for r in results])


def solution(mesh):
    in_specs = (
        P(("grp", "ep"), None),
        P(),
        P(None, "tp"),
        P(None, "tp"),
        P(None, "tp"),
        P(("grp", "ep"), "tp", None),
        P(("grp", "ep"), "tp", None),
        P(("grp", "ep")),
        P("tp"),
        P(None, "tp"),
        P(),
        P(("grp", "ep"), None),
        P(("grp", "ep"), None),
        P("ep", None, "tp"),
        P("ep", None, "tp"),
        P("ep", "tp", None),
    )
    out_specs = (P(("grp", "ep"), "tp"), P(("grp", "ep"), "tp"), P(("grp", "ep"), "tp"))
    body = functools.partial(shards, mesh.shape["tp"], mesh.shape["ep"])
    return jax.shard_map(body, mesh=mesh, in_specs=in_specs, out_specs=out_specs, check_vma=False)
```

```python
import functools

import jax
import jax.numpy as jnp
from jax import lax
from jax.experimental import pallas as pl
from jax.experimental.pallas import tpu as pltpu
from jax.sharding import PartitionSpec as P

HEAD_SIZE = 64
LANES = 128
CORES = 2
epsilon = 1e-06
f32 = jnp.float32
bf16 = jnp.bfloat16


def iota(shape, dim):
    return lax.broadcasted_iota(jnp.int32, shape, dim)


def hops(step, count):
    return min(step % count, -step % count)


def far_first(count):
    return sorted(range(1, count), key=lambda step: -hops(step, count))


def near_first(count):
    return sorted(range(1, count), key=lambda step: hops(step, count))


def nt_dot(left, right):
    return lax.dot_general(left, right, (((1,), (1,)), ((), ())), preferred_element_type=f32)


def kernel(
    n_tp,
    n_ep,
    tok_hbm,
    again_hbm,
    wq_hbm,
    wk_hbm,
    wv_hbm,
    key_hbm,
    val_hbm,
    len_hbm,
    bias_hbm,
    wo_hbm,
    fgain_hbm,
    ids_hbm,
    rw_hbm,
    wg_hbm,
    wu_hbm,
    wd_hbm,
    mixed_ref,
    nk_ref,
    nv_ref,
    tok,
    again,
    wq,
    wk,
    wv,
    key,
    val,
    lens,
    bias,
    wo,
    fgain,
    ids,
    rw,
    wg,
    wu,
    wd,
    rows_pad,
    idp,
    rwp,
    tri,
    place,
    combine,
    hid,
    hg,
    zsend,
    zrecv,
    xg,
    rsend,
    rrecv,
    ysend,
    ret,
    local_sem,
    h_ssem,
    h_rsem,
    z_ssem,
    z_rsem,
    g_ssem,
    g_rsem,
    r_ssem,
    r_rsem,
    y_ssem,
    y_rsem,
    ready,
):
    tp = lax.axis_index("tp")
    ep = lax.axis_index("ep")
    core = lax.rem(ep, CORES)
    chip = ep // CORES
    chips = n_ep // CORES
    seq_rows = tok.shape[0]
    slots = 2 * n_ep

    def copies_of(first, pairs):
        made = [
            pltpu.make_async_copy(source, target, local_sem.at[first + number])
            for number, (source, target) in enumerate(pairs)
        ]
        for copy in made:
            copy.start()
        return made

    c_tok, c_again, c_wq, c_len, c_bias, c_key, c_val = copies_of(
        0,
        (
            (tok_hbm, tok),
            (again_hbm, again),
            (wq_hbm, wq),
            (len_hbm, lens),
            (bias_hbm, bias),
            (key_hbm, key),
            (val_hbm, val),
        ),
    )

    def wrap(number, count):
        return jnp.where(number >= count, number - count, number)

    barrier = pltpu.get_barrier_semaphore()
    column = tp == 0
    topmost = jnp.logical_and(column, ep == 0)
    partner = chip * CORES + (1 - core)
    for step in far_first(n_tp):
        pl.semaphore_signal(barrier, inc=1, device_id={"tp": wrap(tp + step, n_tp)})

    @pl.loop(jnp.where(topmost, n_ep, ep + 1), n_ep)
    def _(above):
        pl.semaphore_signal(barrier, inc=1, device_id={"ep": above})

    @pl.when(jnp.logical_and(column, ep > 0))
    def _():
        pl.semaphore_signal(barrier, inc=1, device_id={"ep": 0})

    def landed(view, sem):
        pltpu.make_async_copy(view, view, sem).wait()

    tri_len = tri.shape[0]
    tri[...] = (iota((tri_len, tri_len), 0) > iota((tri_len, tri_len), 1)).astype(f32).astype(bf16)
    rows_pad[...] = jnp.zeros_like(rows_pad)
    hid[...] = jnp.zeros_like(hid)
    idp[...] = jnp.full(idp.shape, -1.0, f32)
    rwp[...] = jnp.zeros_like(rwp)

    c_tok.wait()
    c_again.wait()
    token_rows = tok[...].astype(f32)
    mean_sq = jnp.mean(token_rows * token_rows, axis=1, keepdims=True)
    normed = (token_rows * lax.rsqrt(mean_sq + epsilon) * again[...]).astype(bf16)
    c_wq.wait()
    queries = jnp.dot(normed, wq[...], preferred_element_type=f32).astype(bf16).astype(f32)
    rows_pad[pl.ds(0, seq_rows), :] = queries * HEAD_SIZE ** (-0.5)
    padded = rows_pad[...]
    pad_rows = padded.shape[0]
    low = iota(padded.shape, 1) < HEAD_SIZE
    turned = pltpu.roll(padded, HEAD_SIZE, axis=1)
    both = jnp.concatenate([jnp.where(low, padded, turned), jnp.where(low, turned, padded)], axis=0)
    cols = key.shape[0]
    wide = jnp.concatenate([both] * (cols // LANES), axis=1)
    own_block = (iota(wide.shape, 1) // HEAD_SIZE) == lax.rem(iota(wide.shape, 0), pad_rows)
    spread = jnp.where(own_block, wide, 0.0).astype(bf16)

    c_len.wait()
    c_bias.wait()
    idp[pl.ds(2, 1), pl.ds(0, seq_rows)] = lens[...].astype(f32)
    len_row = jnp.broadcast_to(idp[pl.ds(2, 1), :], (2 * pad_rows, LANES))
    own_lane = iota(len_row.shape, 1) == lax.rem(iota(len_row.shape, 0), pad_rows)
    len_col = jnp.sum(jnp.where(own_lane, len_row, 0.0), axis=1, keepdims=True)
    bias_col = jnp.where(
        iota((2 * pad_rows, 1), 0) < pad_rows, bias[pl.ds(0, 1), pl.ds(0, 1)], bias[pl.ds(0, 1), pl.ds(1, 1)]
    )

    c_key.wait()
    c_wo, c_wk, c_wv, c_ids, c_rw, c_fgain = copies_of(
        7, ((wo_hbm, wo), (wk_hbm, wk), (wv_hbm, wv), (ids_hbm, ids), (rw_hbm, rw), (fgain_hbm, fgain))
    )
    scores = jnp.dot(spread, key[...], preferred_element_type=f32) + bias_col
    in_cache = iota(scores.shape, 1).astype(f32) < len_col
    log_rest = -(jnp.maximum(scores, 0.0) + jnp.log1p(jnp.exp(-jnp.abs(scores))))
    log_rest = jnp.where(in_cache, log_rest, 0.0)
    cache_len = scores.shape[1]
    chunk_count = cache_len // tri_len
    high = log_rest.astype(bf16)
    rest = (log_rest - high.astype(f32)).astype(bf16)
    stacked = jnp.concatenate(
        [part[:, c * tri_len : (c + 1) * tri_len] for part in (high, rest) for c in range(chunk_count)], axis=0
    )
    within = jnp.dot(stacked, tri[...], preferred_element_type=f32)
    tails = []
    carry = jnp.zeros((2 * pad_rows, 1), f32)
    span = 2 * pad_rows
    for c in reversed(range(chunk_count)):
        inner = within[c * span : (c + 1) * span] + within[(chunk_count + c) * span : (chunk_count + c + 1) * span]
        tails.append(inner + carry)
        carry = carry + inner[:, 0:1] + log_rest[:, c * tri_len : c * tri_len + 1]
    tail = jnp.concatenate(tails[::-1], axis=1)
    breaks = jnp.where(in_cache, jnp.exp(scores + log_rest + tail), 0.0).astype(bf16)
    c_val.wait()
    mixed_values = nt_dot(breaks, val[...])
    mixed_values = jnp.where(own_block, mixed_values, 0.0)
    folded = mixed_values[:, 0:LANES]
    for c in range(1, cols // LANES):
        folded = folded + mixed_values[:, c * LANES : (c + 1) * LANES]
    folded = folded + pltpu.roll(folded, HEAD_SIZE, axis=1)
    heads = jnp.where(low, folded[:pad_rows], folded[pad_rows:]).astype(bf16)
    hg[tp] = heads

    lowest = jnp.where(column, 1, 0)
    pl.semaphore_wait(barrier, (n_tp - 1) + jnp.where(topmost, n_ep - 1, ep - lowest))
    for step in far_first(n_tp):
        pltpu.make_async_remote_copy(
            hg.at[tp], hg.at[tp], h_ssem, h_rsem, device_id={"tp": wrap(tp + step, n_tp)}
        ).start()

    @pl.loop(lowest, jnp.where(topmost, n_ep, ep))
    def _(below):
        pl.semaphore_signal(ready.at[chip], inc=1, device_id={"ep": below})

    c_wg, c_wu, c_wd = copies_of(0, ((wg_hbm, wg), (wu_hbm, wu), (wd_hbm, wd)))
    c_wk.wait()
    c_wv.wait()
    nk_ref[...] = nt_dot(normed, wk[...]).astype(bf16)
    nv_ref[...] = nt_dot(normed, wv[...]).astype(bf16)
    c_ids.wait()
    c_rw.wait()
    top_count = ids.shape[0]
    idp[pl.ds(0, top_count), pl.ds(0, seq_rows)] = ids[...].astype(f32)
    rwp[pl.ds(0, top_count), pl.ds(0, seq_rows)] = rw[...]
    slot_expert = (iota((slots, LANES), 0) // 2).astype(f32)
    slot_rank = lax.rem(iota((slots, LANES), 0), 2).astype(f32)
    hits = [(slot_expert == idp[pl.ds(k, 1), :]).astype(f32) for k in range(top_count)]
    any_hit = sum(hits)
    upper = (iota((LANES, LANES), 0) < iota((LANES, LANES), 1)).astype(f32).astype(bf16)
    before = jnp.dot(any_hit.astype(bf16), upper, preferred_element_type=f32)
    taken = jnp.where(before == slot_rank, 1.0, 0.0)
    place[...] = (any_hit * taken).astype(bf16)
    weighted = sum(hits[k] * rwp[pl.ds(k, 1), :] for k in range(top_count)) * taken
    weighted_t = weighted.T[: combine.shape[0] // 2]
    weighted_high = weighted_t.astype(bf16)
    combine[pl.ds(0, pad_rows), :] = weighted_high
    combine[pl.ds(pad_rows, pad_rows), :] = (weighted_t - weighted_high.astype(f32)).astype(bf16)
    c_fgain.wait()
    own_cols = pl.ds(pl.multiple_of(tp * LANES, LANES), LANES)
    own_tokens = tok[:, own_cols].astype(f32)
    own_gain = fgain[:, own_cols]

    c_wo.wait()
    inverse_sq = 1.0 / (fgain[...] * fgain[...])
    peers = pl.ds(0, n_tp - 1)
    landed(hg.at[peers], h_rsem)
    all_heads = jnp.concatenate([hg[peer] for peer in range(n_tp)], axis=1)
    attn_out = jnp.dot(all_heads, wo[...], preferred_element_type=f32)
    hid[pl.ds(0, seq_rows), :] = own_tokens + attn_out[:seq_rows]
    scaled = (hid[...] * own_gain).astype(bf16)
    outgoing = jnp.dot(place[...], scaled, preferred_element_type=f32).astype(bf16)
    zsend[...] = outgoing.reshape(zsend.shape)

    bounds = (0, n_ep // 4, n_ep)
    own_group = jnp.where(ep >= bounds[1], 1, 0)
    def send_slots(to_ep):
        @pl.when(to_ep != ep)
        def _():
            pltpu.make_async_remote_copy(
                zsend.at[to_ep], zrecv.at[ep], z_ssem, z_rsem.at[own_group], device_id={"ep": to_ep}
            ).start()

    @pl.when(jnp.logical_not(column))
    def _():
        send_slots(0)

    for to_chip in range(chips):
        if to_chip == chips - 1:

            @pl.when(jnp.logical_and(column, ep > 0))
            def _():
                pl.semaphore_wait(ready.at[0], 1)
                send_slots(0)

        @pl.when(jnp.logical_and(to_chip > chip, jnp.logical_not(topmost)))
        def _():
            pl.semaphore_wait(ready.at[to_chip], CORES)

        @pl.when(jnp.logical_and(jnp.logical_and(to_chip == chip, core == 0), jnp.logical_not(topmost)))
        def _():
            pl.semaphore_wait(ready.at[to_chip], 1)

        for to_ep in range(max(1, to_chip * CORES), (to_chip + 1) * CORES):
            send_slots(to_ep)

    pltpu.make_async_copy(zsend.at[ep], zrecv.at[ep], z_rsem.at[own_group]).start()

    c_wg.wait()
    c_wu.wait()
    c_wd.wait()
    groups = tuple(zip(bounds[:-1], bounds[1:]))

    def gather(group):
        first, last = groups[group]
        eps, here = pl.ds(first, last - first), pl.ds(2 * first, 2 * (last - first))
        landed(zrecv.at[eps], z_rsem.at[group])
        xg[tp, here] = zrecv[eps].reshape(2 * (last - first), LANES)
        for step in far_first(n_tp):
            pltpu.make_async_remote_copy(
                xg.at[tp, here],
                xg.at[tp, here],
                g_ssem.at[group],
                g_rsem.at[group],
                device_id={"tp": wrap(tp + step, n_tp)},
            ).start()

    def experts(group):
        first, last = groups[group]
        here = pl.ds(2 * first, 2 * (last - first))
        landed(xg.at[peers, here], g_rsem.at[group])
        rows = jnp.concatenate([xg[peer, here] for peer in range(n_tp)], axis=1)
        gate = jnp.dot(rows, wg[...], preferred_element_type=f32)
        up = jnp.dot(rows, wu[...], preferred_element_type=f32)
        plain = rows.astype(f32)
        sum_sq = jnp.sum(plain * plain * inverse_sq, axis=1, keepdims=True)
        scale = lax.rsqrt(sum_sq / (n_tp * LANES) + epsilon)
        gate = gate * scale
        up = up * scale
        hidden_act = (gate / (1.0 + jnp.exp(-gate)) * up).astype(bf16)
        partial_value = jnp.dot(hidden_act, wd[...], preferred_element_type=f32).astype(bf16)
        for c in range(n_tp):
            rsend[c, here] = partial_value[:, c * LANES : (c + 1) * LANES]
        for step in far_first(n_tp):
            peer = wrap(tp + step, n_tp)
            pltpu.make_async_remote_copy(
                rsend.at[peer, here], rrecv.at[tp, here], r_ssem.at[group], r_rsem.at[group], device_id={"tp": peer}
            ).start()
        rrecv[tp, here] = rsend[tp, here]

    def give_back(group):
        first, last = groups[group]
        eps, here = pl.ds(first, last - first), pl.ds(2 * first, 2 * (last - first))
        landed(rrecv.at[peers, here], r_rsem.at[group])
        total = rrecv[0, here].astype(f32)
        for peer in range(1, n_tp):
            total += rrecv[peer, here].astype(f32)
        ysend[eps] = total.astype(bf16).reshape(last - first, 2, LANES)
        for to_ep in range(first, last):

            @pl.when(to_ep != ep)
            def _():
                pltpu.make_async_remote_copy(
                    ysend.at[to_ep], ret.at[ep], y_ssem, y_rsem, device_id={"ep": to_ep}
                ).start()

    gather(0)
    experts(0)
    gather(1)
    give_back(0)
    experts(1)
    give_back(1)
    pltpu.make_async_copy(ysend.at[ep], ret.at[ep], y_rsem).start()
    landed(ret, y_rsem)
    picked = jnp.dot(combine[...], ret[...].reshape(slots, LANES), preferred_element_type=f32)
    routed_sum = picked[:pad_rows] + picked[pad_rows:]
    mixed_ref[...] = (hid[pl.ds(0, seq_rows), :] + routed_sum[:seq_rows]).astype(bf16)
    landed(hg.at[peers], h_ssem)
    landed(zsend.at[pl.ds(0, n_ep - 1)], z_ssem)
    for group, (first, last) in enumerate(groups):
        here = pl.ds(2 * first, 2 * (last - first))
        landed(xg.at[peers, here], g_ssem.at[group])
        landed(rsend.at[peers, here], r_ssem.at[group])
    landed(ysend.at[pl.ds(0, n_ep - 1)], y_ssem)


def write_out(*refs):
    count = len(refs) // 2
    copies = [pltpu.make_async_copy(refs[n], refs[count + n], refs[-1].at[n]) for n in range(count)]
    for copy in copies:
        copy.start()
    for copy in copies:
        copy.wait()


def shards(
    n_tp,
    n_ep,
    tokens,
    attn_gain,
    w_query,
    w_key,
    w_value,
    key_cache,
    value_cache,
    lengths,
    head_bias,
    w_out,
    ffn_gain,
    route_ids,
    route_weights,
    w_gate,
    w_up,
    w_down,
):
    seq_rows, model_width = tokens.shape
    cache_len = key_cache.shape[2]
    kv_cols = key_cache.shape[1]
    pad_rows = 16
    slots = 2 * n_ep
    operands = (
        tokens,
        attn_gain.reshape(1, model_width),
        w_query,
        w_key.T,
        w_value.T,
        key_cache.reshape(seq_rows * kv_cols, cache_len),
        value_cache.reshape(seq_rows * kv_cols, cache_len),
        lengths.reshape(1, seq_rows),
        head_bias.reshape(1, head_bias.shape[0]),
        w_out,
        ffn_gain.reshape(1, model_width),
        route_ids.T,
        route_weights.T,
        w_gate[0],
        w_up[0],
        w_down[0],
    )
    dma = pltpu.SemaphoreType.DMA
    scratch = [pltpu.VMEM(op.shape, op.dtype) for op in operands] + [
        pltpu.VMEM((pad_rows, LANES), f32),
        pltpu.VMEM((8, LANES), f32),
        pltpu.VMEM((8, LANES), f32),
        pltpu.VMEM((256, 256), bf16),
        pltpu.VMEM((slots, LANES), bf16),
        pltpu.VMEM((2 * pad_rows, slots), bf16),
        pltpu.VMEM((LANES, LANES), f32),
        pltpu.VMEM((n_tp, pad_rows, LANES), bf16),
        pltpu.VMEM((n_ep, 2, LANES), bf16),
        pltpu.VMEM((n_ep, 2, LANES), bf16),
        pltpu.VMEM((n_tp, slots, LANES), bf16),
        pltpu.VMEM((n_tp, slots, LANES), bf16),
        pltpu.VMEM((n_tp, slots, LANES), bf16),
        pltpu.VMEM((n_ep, 2, LANES), bf16),
        pltpu.VMEM((n_ep, 2, LANES), bf16),
        dma((13,)),
        dma,
        dma,
        dma,
        dma((2,)),
        dma((2,)),
        dma((2,)),
        dma((2,)),
        dma((2,)),
        dma,
        dma,
        pltpu.SemaphoreType.REGULAR((n_ep // CORES,)),
    ]
    shapes = (
        (seq_rows, w_out.shape[1]),
        (seq_rows, w_key.shape[1]),
        (seq_rows, w_value.shape[1]),
    )
    results = pl.pallas_call(
        functools.partial(kernel, n_tp, n_ep),
        out_shape=tuple(pltpu.VMEM(shape, bf16) for shape in shapes),
        in_specs=[pl.BlockSpec(memory_space=pltpu.HBM)] * len(operands),
        out_specs=[pl.BlockSpec(memory_space=pltpu.VMEM)] * 3,
        scratch_shapes=scratch,
        compiler_params=pltpu.CompilerParams(collective_id=0, has_side_effects=True),
    )(*operands)
    return pl.pallas_call(
        write_out,
        out_shape=tuple(jax.ShapeDtypeStruct(shape, bf16) for shape in shapes),
        in_specs=[pl.BlockSpec(memory_space=pltpu.VMEM)] * 3,
        out_specs=[pl.BlockSpec(memory_space=pltpu.HBM)] * 3,
        scratch_shapes=[dma((3,))],
    )(*[pltpu.with_memory_space_constraint(r, pltpu.VMEM) for r in results])


def solution(mesh):
    in_specs = (
        P(("grp", "ep"), None),
        P(),
        P(None, "tp"),
        P(None, "tp"),
        P(None, "tp"),
        P(("grp", "ep"), "tp", None),
        P(("grp", "ep"), "tp", None),
        P(("grp", "ep")),
        P("tp"),
        P(None, "tp"),
        P(),
        P(("grp", "ep"), None),
        P(("grp", "ep"), None),
        P("ep", None, "tp"),
        P("ep", None, "tp"),
        P("ep", "tp", None),
    )
    out_specs = (P(("grp", "ep"), "tp"), P(("grp", "ep"), "tp"), P(("grp", "ep"), "tp"))
    body = functools.partial(shards, mesh.shape["tp"], mesh.shape["ep"])
    return jax.shard_map(body, mesh=mesh, in_specs=in_specs, out_specs=out_specs, check_vma=False)
```

```python
import functools

import jax
import jax.numpy as jnp
from jax import lax
from jax.experimental import pallas as pl
from jax.experimental.pallas import tpu as pltpu
from jax.sharding import PartitionSpec as P

HEAD_SIZE = 64
LANES = 128
CORES = 2
ALONE = 8
epsilon = 1e-06
f32 = jnp.float32
bf16 = jnp.bfloat16


def iota(shape, dim):
    return lax.broadcasted_iota(jnp.int32, shape, dim)


def hops(step, count):
    return min(step % count, -step % count)


def far_first(count):
    return sorted(range(1, count), key=lambda step: -hops(step, count))


def near_first(count):
    return sorted(range(1, count), key=lambda step: hops(step, count))


def nt_dot(left, right):
    return lax.dot_general(left, right, (((1,), (1,)), ((), ())), preferred_element_type=f32)


def kernel(
    n_tp,
    n_ep,
    tok_hbm,
    again_hbm,
    wq_hbm,
    wk_hbm,
    wv_hbm,
    key_hbm,
    val_hbm,
    len_hbm,
    bias_hbm,
    wo_hbm,
    fgain_hbm,
    ids_hbm,
    rw_hbm,
    wg_hbm,
    wu_hbm,
    wd_hbm,
    mixed_ref,
    nk_ref,
    nv_ref,
    tok,
    again,
    wq,
    wk,
    wv,
    key,
    val,
    lens,
    bias,
    wo,
    fgain,
    ids,
    rw,
    wg,
    wu,
    wd,
    rows_pad,
    idp,
    rwp,
    tri,
    place,
    combine,
    hid,
    hg,
    zsend,
    zrecv,
    xg,
    rsend,
    rrecv,
    ysend,
    ret,
    local_sem,
    h_ssem,
    h_rsem,
    z_ssem,
    z_rsem,
    g_ssem,
    g_rsem,
    r_ssem,
    r_rsem,
    y_ssem,
    y_rsem,
    ready,
):
    tp = lax.axis_index("tp")
    ep = lax.axis_index("ep")
    core = lax.rem(ep, CORES)
    chip = ep // CORES
    chips = n_ep // CORES
    seq_rows = tok.shape[0]
    slots = 2 * n_ep

    def copies_of(first, pairs):
        made = [
            pltpu.make_async_copy(source, target, local_sem.at[first + number])
            for number, (source, target) in enumerate(pairs)
        ]
        for copy in made:
            copy.start()
        return made

    c_tok, c_again, c_wq, c_len, c_bias, c_key, c_val = copies_of(
        0,
        (
            (tok_hbm, tok),
            (again_hbm, again),
            (wq_hbm, wq),
            (len_hbm, lens),
            (bias_hbm, bias),
            (key_hbm, key),
            (val_hbm, val),
        ),
    )

    def wrap(number, count):
        return jnp.where(number >= count, number - count, number)

    barrier = pltpu.get_barrier_semaphore()
    column = tp == 0
    topmost = jnp.logical_and(column, ep == 0)
    partner = chip * CORES + (1 - core)
    for step in far_first(n_tp):
        pl.semaphore_signal(barrier, inc=1, device_id={"tp": wrap(tp + step, n_tp)})

    @pl.loop(jnp.where(topmost, n_ep, ep + 1), n_ep)
    def _(above):
        pl.semaphore_signal(barrier, inc=1, device_id={"ep": above})

    @pl.when(jnp.logical_and(column, ep > 0))
    def _():
        pl.semaphore_signal(barrier, inc=1, device_id={"ep": 0})

    def landed(view, sem):
        pltpu.make_async_copy(view, view, sem).wait()

    tri_len = tri.shape[0]
    tri[...] = (iota((tri_len, tri_len), 0) > iota((tri_len, tri_len), 1)).astype(f32).astype(bf16)
    rows_pad[...] = jnp.zeros_like(rows_pad)
    hid[...] = jnp.zeros_like(hid)
    zrecv[pl.ds(1, ALONE - 1)] = jnp.zeros((ALONE - 1, 2, LANES), bf16)
    zrecv[ALONE + n_ep // 4 - 1] = jnp.zeros((2, LANES), bf16)
    idp[...] = jnp.full(idp.shape, -1.0, f32)
    rwp[...] = jnp.zeros_like(rwp)

    c_tok.wait()
    c_again.wait()
    token_rows = tok[...].astype(f32)
    mean_sq = jnp.mean(token_rows * token_rows, axis=1, keepdims=True)
    normed = (token_rows * lax.rsqrt(mean_sq + epsilon) * again[...]).astype(bf16)
    c_wq.wait()
    queries = jnp.dot(normed, wq[...], preferred_element_type=f32).astype(bf16).astype(f32)
    rows_pad[pl.ds(0, seq_rows), :] = queries * HEAD_SIZE ** (-0.5)
    padded = rows_pad[...]
    pad_rows = padded.shape[0]
    low = iota(padded.shape, 1) < HEAD_SIZE
    turned = pltpu.roll(padded, HEAD_SIZE, axis=1)
    both = jnp.concatenate([jnp.where(low, padded, turned), jnp.where(low, turned, padded)], axis=0)
    cols = key.shape[0]
    wide = jnp.concatenate([both] * (cols // LANES), axis=1)
    own_block = (iota(wide.shape, 1) // HEAD_SIZE) == lax.rem(iota(wide.shape, 0), pad_rows)
    spread = jnp.where(own_block, wide, 0.0).astype(bf16)

    c_len.wait()
    c_bias.wait()
    idp[pl.ds(2, 1), pl.ds(0, seq_rows)] = lens[...].astype(f32)
    len_row = jnp.broadcast_to(idp[pl.ds(2, 1), :], (2 * pad_rows, LANES))
    own_lane = iota(len_row.shape, 1) == lax.rem(iota(len_row.shape, 0), pad_rows)
    len_col = jnp.sum(jnp.where(own_lane, len_row, 0.0), axis=1, keepdims=True)
    bias_col = jnp.where(
        iota((2 * pad_rows, 1), 0) < pad_rows, bias[pl.ds(0, 1), pl.ds(0, 1)], bias[pl.ds(0, 1), pl.ds(1, 1)]
    )

    c_key.wait()
    c_wo, c_wk, c_wv, c_ids, c_rw, c_fgain = copies_of(
        7, ((wo_hbm, wo), (wk_hbm, wk), (wv_hbm, wv), (ids_hbm, ids), (rw_hbm, rw), (fgain_hbm, fgain))
    )
    scores = jnp.dot(spread, key[...], preferred_element_type=f32) + bias_col
    in_cache = iota(scores.shape, 1).astype(f32) < len_col
    log_rest = -(jnp.maximum(scores, 0.0) + jnp.log1p(jnp.exp(-jnp.abs(scores))))
    log_rest = jnp.where(in_cache, log_rest, 0.0)
    cache_len = scores.shape[1]
    chunk_count = cache_len // tri_len
    high = log_rest.astype(bf16)
    rest = (log_rest - high.astype(f32)).astype(bf16)
    stacked = jnp.concatenate(
        [part[:, c * tri_len : (c + 1) * tri_len] for part in (high, rest) for c in range(chunk_count)], axis=0
    )
    within = jnp.dot(stacked, tri[...], preferred_element_type=f32)
    tails = []
    carry = jnp.zeros((2 * pad_rows, 1), f32)
    span = 2 * pad_rows
    for c in reversed(range(chunk_count)):
        inner = within[c * span : (c + 1) * span] + within[(chunk_count + c) * span : (chunk_count + c + 1) * span]
        tails.append(inner + carry)
        carry = carry + inner[:, 0:1] + log_rest[:, c * tri_len : c * tri_len + 1]
    tail = jnp.concatenate(tails[::-1], axis=1)
    breaks = jnp.where(in_cache, jnp.exp(scores + log_rest + tail), 0.0).astype(bf16)
    c_val.wait()
    mixed_values = nt_dot(breaks, val[...])
    mixed_values = jnp.where(own_block, mixed_values, 0.0)
    folded = mixed_values[:, 0:LANES]
    for c in range(1, cols // LANES):
        folded = folded + mixed_values[:, c * LANES : (c + 1) * LANES]
    folded = folded + pltpu.roll(folded, HEAD_SIZE, axis=1)
    heads = jnp.where(low, folded[:pad_rows], folded[pad_rows:]).astype(bf16)
    hg[tp] = heads

    lowest = jnp.where(column, 1, 0)
    pl.semaphore_wait(barrier, (n_tp - 1) + jnp.where(topmost, n_ep - 1, ep - lowest))
    for step in far_first(n_tp):
        pltpu.make_async_remote_copy(
            hg.at[tp], hg.at[tp], h_ssem, h_rsem, device_id={"tp": wrap(tp + step, n_tp)}
        ).start()

    @pl.loop(lowest, jnp.where(topmost, n_ep, ep))
    def _(below):
        pl.semaphore_signal(ready.at[chip], inc=1, device_id={"ep": below})

    c_wg, c_wu, c_wd = copies_of(0, ((wg_hbm, wg), (wu_hbm, wu), (wd_hbm, wd)))
    c_wk.wait()
    c_wv.wait()
    nk_ref[...] = nt_dot(normed, wk[...]).astype(bf16)
    nv_ref[...] = nt_dot(normed, wv[...]).astype(bf16)
    c_ids.wait()
    c_rw.wait()
    top_count = ids.shape[0]
    idp[pl.ds(0, top_count), pl.ds(0, seq_rows)] = ids[...].astype(f32)
    rwp[pl.ds(0, top_count), pl.ds(0, seq_rows)] = rw[...]
    slot_expert = (iota((slots, LANES), 0) // 2).astype(f32)
    slot_rank = lax.rem(iota((slots, LANES), 0), 2).astype(f32)
    hits = [(slot_expert == idp[pl.ds(k, 1), :]).astype(f32) for k in range(top_count)]
    any_hit = sum(hits)
    upper = (iota((LANES, LANES), 0) < iota((LANES, LANES), 1)).astype(f32).astype(bf16)
    before = jnp.dot(any_hit.astype(bf16), upper, preferred_element_type=f32)
    taken = jnp.where(before == slot_rank, 1.0, 0.0)
    place[...] = (any_hit * taken).astype(bf16)
    weighted = sum(hits[k] * rwp[pl.ds(k, 1), :] for k in range(top_count)) * taken
    weighted_t = weighted.T[: combine.shape[0] // 2]
    weighted_high = weighted_t.astype(bf16)
    combine[pl.ds(0, pad_rows), :] = weighted_high
    combine[pl.ds(pad_rows, pad_rows), :] = (weighted_t - weighted_high.astype(f32)).astype(bf16)
    c_fgain.wait()
    own_cols = pl.ds(pl.multiple_of(tp * LANES, LANES), LANES)
    own_tokens = tok[:, own_cols].astype(f32)
    own_gain = fgain[:, own_cols]

    c_wo.wait()
    inverse_sq = 1.0 / (fgain[...] * fgain[...])
    peers = pl.ds(0, n_tp - 1)
    landed(hg.at[peers], h_rsem)
    all_heads = jnp.concatenate([hg[peer] for peer in range(n_tp)], axis=1)
    attn_out = jnp.dot(all_heads, wo[...], preferred_element_type=f32)
    hid[pl.ds(0, seq_rows), :] = own_tokens + attn_out[:seq_rows]
    scaled = (hid[...] * own_gain).astype(bf16)
    outgoing = jnp.dot(place[...], scaled, preferred_element_type=f32).astype(bf16)
    zsend[...] = outgoing.reshape(zsend.shape)

    quarter = n_ep // 4
    groups = ((0, 1, 0, ALONE), (1, quarter, ALONE, quarter), (quarter, n_ep, ALONE + quarter, n_ep - quarter))
    own_group = jnp.where(ep == 0, 0, jnp.where(ep < quarter, 1, 2))
    own_entry = jnp.where(ep == 0, 0, jnp.where(ep < quarter, ep + (ALONE - 1), ep + ALONE))
    def send_slots(to_ep):
        @pl.when(to_ep != ep)
        def _():
            pltpu.make_async_remote_copy(
                zsend.at[to_ep], zrecv.at[own_entry], z_ssem, z_rsem.at[own_group], device_id={"ep": to_ep}
            ).start()

    @pl.when(jnp.logical_not(column))
    def _():
        send_slots(0)

    for to_chip in range(chips):
        if to_chip == chips - 1:

            @pl.when(jnp.logical_and(column, ep > 0))
            def _():
                pl.semaphore_wait(ready.at[0], 1)
                send_slots(0)

        @pl.when(jnp.logical_and(to_chip > chip, jnp.logical_not(topmost)))
        def _():
            pl.semaphore_wait(ready.at[to_chip], CORES)

        @pl.when(jnp.logical_and(jnp.logical_and(to_chip == chip, core == 0), jnp.logical_not(topmost)))
        def _():
            pl.semaphore_wait(ready.at[to_chip], 1)

        for to_ep in range(max(1, to_chip * CORES), (to_chip + 1) * CORES):
            send_slots(to_ep)

    pltpu.make_async_copy(zsend.at[ep], zrecv.at[own_entry], z_rsem.at[own_group]).start()

    c_wg.wait()
    c_wu.wait()
    c_wd.wait()
    def gather(group):
        first, last, entry, width = groups[group]
        here = pl.ds(2 * entry, 2 * width)
        landed(zrecv.at[pl.ds(entry, last - first)], z_rsem.at[group])
        xg[tp, here] = zrecv[pl.ds(entry, width)].reshape(2 * width, LANES)
        for step in far_first(n_tp):
            pltpu.make_async_remote_copy(
                xg.at[tp, here],
                xg.at[tp, here],
                g_ssem.at[group],
                g_rsem.at[group],
                device_id={"tp": wrap(tp + step, n_tp)},
            ).start()

    def experts(group):
        here = pl.ds(2 * groups[group][2], 2 * groups[group][3])
        landed(xg.at[peers, here], g_rsem.at[group])
        rows = jnp.concatenate([xg[peer, here] for peer in range(n_tp)], axis=1)
        gate = jnp.dot(rows, wg[...], preferred_element_type=f32)
        up = jnp.dot(rows, wu[...], preferred_element_type=f32)
        plain = rows.astype(f32)
        sum_sq = jnp.sum(plain * plain * inverse_sq, axis=1, keepdims=True)
        scale = lax.rsqrt(sum_sq / (n_tp * LANES) + epsilon)
        gate = gate * scale
        up = up * scale
        hidden_act = (gate / (1.0 + jnp.exp(-gate)) * up).astype(bf16)
        partial_value = jnp.dot(hidden_act, wd[...], preferred_element_type=f32).astype(bf16)
        for c in range(n_tp):
            rsend[c, here] = partial_value[:, c * LANES : (c + 1) * LANES]
        for step in far_first(n_tp):
            peer = wrap(tp + step, n_tp)
            pltpu.make_async_remote_copy(
                rsend.at[peer, here], rrecv.at[tp, here], r_ssem.at[group], r_rsem.at[group], device_id={"tp": peer}
            ).start()
        rrecv[tp, here] = rsend[tp, here]

    def give_back(group):
        first, last, entry, width = groups[group]
        here = pl.ds(2 * entry, 2 * width)
        landed(rrecv.at[peers, here], r_rsem.at[group])
        total = rrecv[0, here].astype(f32)
        for peer in range(1, n_tp):
            total += rrecv[peer, here].astype(f32)
        ysend[pl.ds(entry, width)] = total.astype(bf16).reshape(width, 2, LANES)
        for to_ep in range(first, last):

            @pl.when(to_ep != ep)
            def _():
                pltpu.make_async_remote_copy(
                    ysend.at[entry + to_ep - first], ret.at[ep], y_ssem, y_rsem, device_id={"ep": to_ep}
                ).start()

    gather(1)
    gather(0)
    experts(1)
    experts(0)
    gather(2)
    give_back(1)
    give_back(0)
    experts(2)
    give_back(2)
    pltpu.make_async_copy(ysend.at[own_entry], ret.at[ep], y_rsem).start()
    landed(ret, y_rsem)
    picked = jnp.dot(combine[...], ret[...].reshape(slots, LANES), preferred_element_type=f32)
    routed_sum = picked[:pad_rows] + picked[pad_rows:]
    mixed_ref[...] = (hid[pl.ds(0, seq_rows), :] + routed_sum[:seq_rows]).astype(bf16)
    landed(hg.at[peers], h_ssem)
    landed(zsend.at[pl.ds(0, n_ep - 1)], z_ssem)
    for group, (_, _, entry, width) in enumerate(groups):
        here = pl.ds(2 * entry, 2 * width)
        landed(xg.at[peers, here], g_ssem.at[group])
        landed(rsend.at[peers, here], r_ssem.at[group])
    landed(ysend.at[pl.ds(0, n_ep - 1)], y_ssem)


def write_out(*refs):
    count = len(refs) // 2
    copies = [pltpu.make_async_copy(refs[n], refs[count + n], refs[-1].at[n]) for n in range(count)]
    for copy in copies:
        copy.start()
    for copy in copies:
        copy.wait()


def shards(
    n_tp,
    n_ep,
    tokens,
    attn_gain,
    w_query,
    w_key,
    w_value,
    key_cache,
    value_cache,
    lengths,
    head_bias,
    w_out,
    ffn_gain,
    route_ids,
    route_weights,
    w_gate,
    w_up,
    w_down,
):
    seq_rows, model_width = tokens.shape
    cache_len = key_cache.shape[2]
    kv_cols = key_cache.shape[1]
    pad_rows = 16
    slots = 2 * n_ep
    operands = (
        tokens,
        attn_gain.reshape(1, model_width),
        w_query,
        w_key.T,
        w_value.T,
        key_cache.reshape(seq_rows * kv_cols, cache_len),
        value_cache.reshape(seq_rows * kv_cols, cache_len),
        lengths.reshape(1, seq_rows),
        head_bias.reshape(1, head_bias.shape[0]),
        w_out,
        ffn_gain.reshape(1, model_width),
        route_ids.T,
        route_weights.T,
        w_gate[0],
        w_up[0],
        w_down[0],
    )
    dma = pltpu.SemaphoreType.DMA
    scratch = [pltpu.VMEM(op.shape, op.dtype) for op in operands] + [
        pltpu.VMEM((pad_rows, LANES), f32),
        pltpu.VMEM((8, LANES), f32),
        pltpu.VMEM((8, LANES), f32),
        pltpu.VMEM((256, 256), bf16),
        pltpu.VMEM((slots, LANES), bf16),
        pltpu.VMEM((2 * pad_rows, slots), bf16),
        pltpu.VMEM((LANES, LANES), f32),
        pltpu.VMEM((n_tp, pad_rows, LANES), bf16),
        pltpu.VMEM((n_ep, 2, LANES), bf16),
        pltpu.VMEM((n_ep + ALONE, 2, LANES), bf16),
        pltpu.VMEM((n_tp, slots + 2 * ALONE, LANES), bf16),
        pltpu.VMEM((n_tp, slots + 2 * ALONE, LANES), bf16),
        pltpu.VMEM((n_tp, slots + 2 * ALONE, LANES), bf16),
        pltpu.VMEM((n_ep + ALONE, 2, LANES), bf16),
        pltpu.VMEM((n_ep, 2, LANES), bf16),
        dma((13,)),
        dma,
        dma,
        dma,
        dma((3,)),
        dma((3,)),
        dma((3,)),
        dma((3,)),
        dma((3,)),
        dma,
        dma,
        pltpu.SemaphoreType.REGULAR((n_ep // CORES,)),
    ]
    shapes = (
        (seq_rows, w_out.shape[1]),
        (seq_rows, w_key.shape[1]),
        (seq_rows, w_value.shape[1]),
    )
    results = pl.pallas_call(
        functools.partial(kernel, n_tp, n_ep),
        out_shape=tuple(pltpu.VMEM(shape, bf16) for shape in shapes),
        in_specs=[pl.BlockSpec(memory_space=pltpu.HBM)] * len(operands),
        out_specs=[pl.BlockSpec(memory_space=pltpu.VMEM)] * 3,
        scratch_shapes=scratch,
        compiler_params=pltpu.CompilerParams(collective_id=0, has_side_effects=True),
    )(*operands)
    return pl.pallas_call(
        write_out,
        out_shape=tuple(jax.ShapeDtypeStruct(shape, bf16) for shape in shapes),
        in_specs=[pl.BlockSpec(memory_space=pltpu.VMEM)] * 3,
        out_specs=[pl.BlockSpec(memory_space=pltpu.HBM)] * 3,
        scratch_shapes=[dma((3,))],
    )(*[pltpu.with_memory_space_constraint(r, pltpu.VMEM) for r in results])


def solution(mesh):
    in_specs = (
        P(("grp", "ep"), None),
        P(),
        P(None, "tp"),
        P(None, "tp"),
        P(None, "tp"),
        P(("grp", "ep"), "tp", None),
        P(("grp", "ep"), "tp", None),
        P(("grp", "ep")),
        P("tp"),
        P(None, "tp"),
        P(),
        P(("grp", "ep"), None),
        P(("grp", "ep"), None),
        P("ep", None, "tp"),
        P("ep", None, "tp"),
        P("ep", "tp", None),
    )
    out_specs = (P(("grp", "ep"), "tp"), P(("grp", "ep"), "tp"), P(("grp", "ep"), "tp"))
    body = functools.partial(shards, mesh.shape["tp"], mesh.shape["ep"])
    return jax.shard_map(body, mesh=mesh, in_specs=in_specs, out_specs=out_specs, check_vma=False)
```

```python
import functools

import jax
import jax.numpy as jnp
from jax import lax
from jax.experimental import pallas as pl
from jax.experimental.pallas import tpu as pltpu
from jax.sharding import PartitionSpec as P

HEAD_SIZE = 64
LANES = 128
CORES = 2
ALONE = 8
epsilon = 1e-06
f32 = jnp.float32
bf16 = jnp.bfloat16


def iota(shape, dim):
    return lax.broadcasted_iota(jnp.int32, shape, dim)


def hops(step, count):
    return min(step % count, -step % count)


def far_first(count):
    return sorted(range(1, count), key=lambda step: -hops(step, count))


def near_first(count):
    return sorted(range(1, count), key=lambda step: hops(step, count))


def nt_dot(left, right):
    return lax.dot_general(left, right, (((1,), (1,)), ((), ())), preferred_element_type=f32)


def kernel(
    n_tp,
    n_ep,
    tok_hbm,
    again_hbm,
    wq_hbm,
    wk_hbm,
    wv_hbm,
    key_hbm,
    val_hbm,
    len_hbm,
    bias_hbm,
    wo_hbm,
    fgain_hbm,
    ids_hbm,
    rw_hbm,
    wg_hbm,
    wu_hbm,
    wd_hbm,
    mixed_ref,
    nk_ref,
    nv_ref,
    tok,
    again,
    wq,
    wk,
    wv,
    key,
    val,
    lens,
    bias,
    wo,
    fgain,
    ids,
    rw,
    wg,
    wu,
    wd,
    rows_pad,
    idp,
    rwp,
    tri,
    place,
    combine,
    hid,
    hg,
    zsend,
    zrecv,
    xg,
    rsend,
    rrecv,
    ysend,
    ret,
    local_sem,
    h_ssem,
    h_rsem,
    z_ssem,
    z_rsem,
    g_ssem,
    g_rsem,
    r_ssem,
    r_rsem,
    y_ssem,
    y_rsem,
    ready,
    psend,
    terms,
    p_ssem,
    p_rsem,
):
    tp = lax.axis_index("tp")
    ep = lax.axis_index("ep")
    core = lax.rem(ep, CORES)
    chip = ep // CORES
    chips = n_ep // CORES
    seq_rows = tok.shape[0]
    slots = 2 * n_ep

    def copies_of(first, pairs):
        made = [
            pltpu.make_async_copy(source, target, local_sem.at[first + number])
            for number, (source, target) in enumerate(pairs)
        ]
        for copy in made:
            copy.start()
        return made

    c_tok, c_again, c_wq, c_len, c_bias, c_key, c_val = copies_of(
        0,
        (
            (tok_hbm, tok),
            (again_hbm, again),
            (wq_hbm, wq),
            (len_hbm, lens),
            (bias_hbm, bias),
            (key_hbm, key),
            (val_hbm, val),
        ),
    )

    def wrap(number, count):
        return jnp.where(number >= count, number - count, number)

    barrier = pltpu.get_barrier_semaphore()
    column = tp == 0
    topmost = jnp.logical_and(column, ep == 0)
    partner = chip * CORES + (1 - core)
    for step in far_first(n_tp):
        pl.semaphore_signal(barrier, inc=1, device_id={"tp": wrap(tp + step, n_tp)})

    @pl.loop(jnp.where(topmost, n_ep, ep + 1), n_ep)
    def _(above):
        pl.semaphore_signal(barrier, inc=1, device_id={"ep": above})

    @pl.when(jnp.logical_and(column, ep > 0))
    def _():
        pl.semaphore_signal(barrier, inc=1, device_id={"ep": 0})

    def landed(view, sem):
        pltpu.make_async_copy(view, view, sem).wait()

    tri_len = tri.shape[0]
    tri[...] = (iota((tri_len, tri_len), 0) > iota((tri_len, tri_len), 1)).astype(f32).astype(bf16)
    rows_pad[...] = jnp.zeros_like(rows_pad)
    hid[...] = jnp.zeros_like(hid)
    zrecv[pl.ds(1, ALONE - 1)] = jnp.zeros((ALONE - 1, 2, LANES), bf16)
    zrecv[ALONE + n_ep // 4 - 1] = jnp.zeros((2, LANES), bf16)
    idp[...] = jnp.full(idp.shape, -1.0, f32)
    rwp[...] = jnp.zeros_like(rwp)

    c_tok.wait()
    c_again.wait()
    token_rows = tok[...].astype(f32)
    mean_sq = jnp.mean(token_rows * token_rows, axis=1, keepdims=True)
    normed = (token_rows * lax.rsqrt(mean_sq + epsilon) * again[...]).astype(bf16)
    c_wq.wait()
    queries = jnp.dot(normed, wq[...], preferred_element_type=f32).astype(bf16).astype(f32)
    rows_pad[pl.ds(0, seq_rows), :] = queries * HEAD_SIZE ** (-0.5)
    padded = rows_pad[...]
    pad_rows = padded.shape[0]
    low = iota(padded.shape, 1) < HEAD_SIZE
    turned = pltpu.roll(padded, HEAD_SIZE, axis=1)
    both = jnp.concatenate([jnp.where(low, padded, turned), jnp.where(low, turned, padded)], axis=0)
    cols = key.shape[0]
    wide = jnp.concatenate([both] * (cols // LANES), axis=1)
    own_block = (iota(wide.shape, 1) // HEAD_SIZE) == lax.rem(iota(wide.shape, 0), pad_rows)
    spread = jnp.where(own_block, wide, 0.0).astype(bf16)

    c_len.wait()
    c_bias.wait()
    idp[pl.ds(2, 1), pl.ds(0, seq_rows)] = lens[...].astype(f32)
    len_row = jnp.broadcast_to(idp[pl.ds(2, 1), :], (2 * pad_rows, LANES))
    own_lane = iota(len_row.shape, 1) == lax.rem(iota(len_row.shape, 0), pad_rows)
    len_col = jnp.sum(jnp.where(own_lane, len_row, 0.0), axis=1, keepdims=True)
    bias_col = jnp.where(
        iota((2 * pad_rows, 1), 0) < pad_rows, bias[pl.ds(0, 1), pl.ds(0, 1)], bias[pl.ds(0, 1), pl.ds(1, 1)]
    )

    c_key.wait()
    c_wo, c_wk, c_wv, c_ids, c_rw, c_fgain = copies_of(
        7, ((wo_hbm, wo), (wk_hbm, wk), (wv_hbm, wv), (ids_hbm, ids), (rw_hbm, rw), (fgain_hbm, fgain))
    )
    scores = jnp.dot(spread, key[...], preferred_element_type=f32) + bias_col
    in_cache = iota(scores.shape, 1).astype(f32) < len_col
    log_rest = -(jnp.maximum(scores, 0.0) + jnp.log1p(jnp.exp(-jnp.abs(scores))))
    log_rest = jnp.where(in_cache, log_rest, 0.0)
    cache_len = scores.shape[1]
    chunk_count = cache_len // tri_len
    high = log_rest.astype(bf16)
    rest = (log_rest - high.astype(f32)).astype(bf16)
    stacked = jnp.concatenate(
        [part[:, c * tri_len : (c + 1) * tri_len] for part in (high, rest) for c in range(chunk_count)], axis=0
    )
    within = jnp.dot(stacked, tri[...], preferred_element_type=f32)
    tails = []
    carry = jnp.zeros((2 * pad_rows, 1), f32)
    span = 2 * pad_rows
    for c in reversed(range(chunk_count)):
        inner = within[c * span : (c + 1) * span] + within[(chunk_count + c) * span : (chunk_count + c + 1) * span]
        tails.append(inner + carry)
        carry = carry + inner[:, 0:1] + log_rest[:, c * tri_len : c * tri_len + 1]
    tail = jnp.concatenate(tails[::-1], axis=1)
    breaks = jnp.where(in_cache, jnp.exp(scores + log_rest + tail), 0.0).astype(bf16)
    c_val.wait()
    mixed_values = nt_dot(breaks, val[...])
    mixed_values = jnp.where(own_block, mixed_values, 0.0)
    folded = mixed_values[:, 0:LANES]
    for c in range(1, cols // LANES):
        folded = folded + mixed_values[:, c * LANES : (c + 1) * LANES]
    folded = folded + pltpu.roll(folded, HEAD_SIZE, axis=1)
    heads = jnp.where(low, folded[:pad_rows], folded[pad_rows:]).astype(bf16)
    hg[tp] = heads

    lowest = jnp.where(column, 1, 0)
    pl.semaphore_wait(barrier, (n_tp - 1) + jnp.where(topmost, n_ep - 1, ep - lowest))
    for step in far_first(n_tp):
        pltpu.make_async_remote_copy(
            hg.at[tp], hg.at[tp], h_ssem, h_rsem, device_id={"tp": wrap(tp + step, n_tp)}
        ).start()

    @pl.loop(lowest, jnp.where(topmost, n_ep, ep))
    def _(below):
        pl.semaphore_signal(ready.at[chip], inc=1, device_id={"ep": below})

    c_wg, c_wu, c_wd = copies_of(0, ((wg_hbm, wg), (wu_hbm, wu), (wd_hbm, wd)))
    c_wk.wait()
    c_wv.wait()
    nk_ref[...] = nt_dot(normed, wk[...]).astype(bf16)
    nv_ref[...] = nt_dot(normed, wv[...]).astype(bf16)
    c_ids.wait()
    c_rw.wait()
    top_count = ids.shape[0]
    idp[pl.ds(0, top_count), pl.ds(0, seq_rows)] = ids[...].astype(f32)
    rwp[pl.ds(0, top_count), pl.ds(0, seq_rows)] = rw[...]
    slot_expert = (iota((slots, LANES), 0) // 2).astype(f32)
    slot_rank = lax.rem(iota((slots, LANES), 0), 2).astype(f32)
    hits = [(slot_expert == idp[pl.ds(k, 1), :]).astype(f32) for k in range(top_count)]
    any_hit = sum(hits)
    upper = (iota((LANES, LANES), 0) < iota((LANES, LANES), 1)).astype(f32).astype(bf16)
    before = jnp.dot(any_hit.astype(bf16), upper, preferred_element_type=f32)
    taken = jnp.where(before == slot_rank, 1.0, 0.0)
    place[...] = (any_hit * taken).astype(bf16)
    weighted = sum(hits[k] * rwp[pl.ds(k, 1), :] for k in range(top_count)) * taken
    weighted_t = weighted.T[: combine.shape[0] // 2]
    weighted_high = weighted_t.astype(bf16)
    combine[pl.ds(0, pad_rows), :] = weighted_high
    combine[pl.ds(pad_rows, pad_rows), :] = (weighted_t - weighted_high.astype(f32)).astype(bf16)
    c_fgain.wait()
    own_cols = pl.ds(pl.multiple_of(tp * LANES, LANES), LANES)
    own_tokens = tok[:, own_cols].astype(f32)
    own_gain = fgain[:, own_cols]

    c_wo.wait()
    inverse_sq = 1.0 / (fgain[...] * fgain[...])
    peers = pl.ds(0, n_tp - 1)
    landed(hg.at[peers], h_rsem)
    all_heads = jnp.concatenate([hg[peer] for peer in range(n_tp)], axis=1)
    attn_out = jnp.dot(all_heads, wo[...], preferred_element_type=f32)
    hid[pl.ds(0, seq_rows), :] = own_tokens + attn_out[:seq_rows]
    scaled = (hid[...] * own_gain).astype(bf16)
    outgoing = jnp.dot(place[...], scaled, preferred_element_type=f32).astype(bf16)
    zsend[...] = outgoing.reshape(zsend.shape)

    quarter = n_ep // 4
    groups = ((0, 1, 0, ALONE), (1, quarter, ALONE, quarter), (quarter, n_ep, ALONE + quarter, n_ep - quarter))
    own_group = jnp.where(ep == 0, 0, jnp.where(ep < quarter, 1, 2))
    own_entry = jnp.where(ep == 0, 0, jnp.where(ep < quarter, ep + (ALONE - 1), ep + ALONE))
    def send_slots(to_ep):
        @pl.when(to_ep != ep)
        def _():
            pltpu.make_async_remote_copy(
                zsend.at[to_ep], zrecv.at[own_entry], z_ssem, z_rsem.at[own_group], device_id={"ep": to_ep}
            ).start()

    @pl.when(jnp.logical_not(column))
    def _():
        send_slots(0)

    for to_chip in range(chips):
        if to_chip == chips - 1:

            @pl.when(jnp.logical_and(column, ep > 0))
            def _():
                pl.semaphore_wait(ready.at[0], 1)
                send_slots(0)

        @pl.when(jnp.logical_and(to_chip > chip, jnp.logical_not(topmost)))
        def _():
            pl.semaphore_wait(ready.at[to_chip], CORES)

        @pl.when(jnp.logical_and(jnp.logical_and(to_chip == chip, core == 0), jnp.logical_not(topmost)))
        def _():
            pl.semaphore_wait(ready.at[to_chip], 1)

        for to_ep in range(max(1, to_chip * CORES), (to_chip + 1) * CORES):
            send_slots(to_ep)

    pltpu.make_async_copy(zsend.at[ep], zrecv.at[own_entry], z_rsem.at[own_group]).start()

    c_wg.wait()
    c_wu.wait()
    c_wd.wait()
    def gather(group):
        first, last, entry, width = groups[group]
        here = pl.ds(2 * entry, 2 * width)
        landed(zrecv.at[pl.ds(entry, last - first)], z_rsem.at[group])
        xg[tp, here] = zrecv[pl.ds(entry, width)].reshape(2 * width, LANES)
        for step in far_first(n_tp):
            pltpu.make_async_remote_copy(
                xg.at[tp, here],
                xg.at[tp, here],
                g_ssem.at[group],
                g_rsem.at[group],
                device_id={"tp": wrap(tp + step, n_tp)},
            ).start()

    def experts(group):
        here = pl.ds(2 * groups[group][2], 2 * groups[group][3])
        landed(xg.at[peers, here], g_rsem.at[group])
        rows = jnp.concatenate([xg[peer, here] for peer in range(n_tp)], axis=1)
        gate = jnp.dot(rows, wg[...], preferred_element_type=f32)
        up = jnp.dot(rows, wu[...], preferred_element_type=f32)
        plain = rows.astype(f32)
        sum_sq = jnp.sum(plain * plain * inverse_sq, axis=1, keepdims=True)
        scale = lax.rsqrt(sum_sq / (n_tp * LANES) + epsilon)
        gate = gate * scale
        up = up * scale
        hidden_act = (gate / (1.0 + jnp.exp(-gate)) * up).astype(bf16)
        partial_value = jnp.dot(hidden_act, wd[...], preferred_element_type=f32).astype(bf16)
        if group == 0:
            for c in range(n_tp):
                psend[c] = partial_value[:2, c * LANES : (c + 1) * LANES]
            for step in far_first(n_tp):
                peer = wrap(tp + step, n_tp)
                pltpu.make_async_remote_copy(
                    psend.at[peer], terms.at[tp, ep], p_ssem, p_rsem, device_id={"ep": 0, "tp": peer}
                ).start()

            @pl.when(ep > 0)
            def _():
                pltpu.make_async_remote_copy(
                    psend.at[tp], terms.at[tp, ep], p_ssem, p_rsem, device_id={"ep": 0}
                ).start()

            @pl.when(ep == 0)
            def _():
                pltpu.make_async_copy(psend.at[tp], terms.at[tp, ep], p_rsem).start()

            return
        for c in range(n_tp):
            rsend[c, here] = partial_value[:, c * LANES : (c + 1) * LANES]
        for step in far_first(n_tp):
            peer = wrap(tp + step, n_tp)
            pltpu.make_async_remote_copy(
                rsend.at[peer, here], rrecv.at[tp, here], r_ssem.at[group], r_rsem.at[group], device_id={"tp": peer}
            ).start()
        rrecv[tp, here] = rsend[tp, here]

    def give_back(group):
        first, last, entry, width = groups[group]
        here = pl.ds(2 * entry, 2 * width)
        landed(rrecv.at[peers, here], r_rsem.at[group])
        total = rrecv[0, here].astype(f32)
        for peer in range(1, n_tp):
            total += rrecv[peer, here].astype(f32)
        ysend[pl.ds(entry, width)] = total.astype(bf16).reshape(width, 2, LANES)
        for to_ep in range(first, last):

            @pl.when(to_ep != ep)
            def _():
                pltpu.make_async_remote_copy(
                    ysend.at[entry + to_ep - first], ret.at[ep], y_ssem, y_rsem, device_id={"ep": to_ep}
                ).start()

    gather(1)
    gather(0)
    experts(1)
    experts(0)
    gather(2)
    give_back(1)
    experts(2)
    give_back(2)
    @pl.when(ep > 0)
    def _():
        pltpu.make_async_copy(ysend.at[own_entry], ret.at[ep], y_rsem).start()
        landed(ret, y_rsem)

    @pl.when(ep == 0)
    def _():
        landed(terms, p_rsem)
        total = terms[0].astype(f32)
        for peer in range(1, n_tp):
            total += terms[peer].astype(f32)
        ret[...] = total.astype(bf16)

    picked = jnp.dot(combine[...], ret[...].reshape(slots, LANES), preferred_element_type=f32)
    routed_sum = picked[:pad_rows] + picked[pad_rows:]
    mixed_ref[...] = (hid[pl.ds(0, seq_rows), :] + routed_sum[:seq_rows]).astype(bf16)
    landed(hg.at[peers], h_ssem)
    landed(zsend.at[pl.ds(0, n_ep - 1)], z_ssem)
    for group, (_, _, entry, width) in enumerate(groups):
        here = pl.ds(2 * entry, 2 * width)
        landed(xg.at[peers, here], g_ssem.at[group])
        if group:
            landed(rsend.at[peers, here], r_ssem.at[group])

    @pl.when(ep > 0)
    def _():
        landed(psend, p_ssem)
        landed(ysend.at[pl.ds(0, n_ep - 2)], y_ssem)

    @pl.when(ep == 0)
    def _():
        landed(psend.at[peers], p_ssem)
        landed(ysend.at[pl.ds(0, n_ep - 1)], y_ssem)


def write_out(*refs):
    count = len(refs) // 2
    copies = [pltpu.make_async_copy(refs[n], refs[count + n], refs[-1].at[n]) for n in range(count)]
    for copy in copies:
        copy.start()
    for copy in copies:
        copy.wait()


def shards(
    n_tp,
    n_ep,
    tokens,
    attn_gain,
    w_query,
    w_key,
    w_value,
    key_cache,
    value_cache,
    lengths,
    head_bias,
    w_out,
    ffn_gain,
    route_ids,
    route_weights,
    w_gate,
    w_up,
    w_down,
):
    seq_rows, model_width = tokens.shape
    cache_len = key_cache.shape[2]
    kv_cols = key_cache.shape[1]
    pad_rows = 16
    slots = 2 * n_ep
    operands = (
        tokens,
        attn_gain.reshape(1, model_width),
        w_query,
        w_key.T,
        w_value.T,
        key_cache.reshape(seq_rows * kv_cols, cache_len),
        value_cache.reshape(seq_rows * kv_cols, cache_len),
        lengths.reshape(1, seq_rows),
        head_bias.reshape(1, head_bias.shape[0]),
        w_out,
        ffn_gain.reshape(1, model_width),
        route_ids.T,
        route_weights.T,
        w_gate[0],
        w_up[0],
        w_down[0],
    )
    dma = pltpu.SemaphoreType.DMA
    scratch = [pltpu.VMEM(op.shape, op.dtype) for op in operands] + [
        pltpu.VMEM((pad_rows, LANES), f32),
        pltpu.VMEM((8, LANES), f32),
        pltpu.VMEM((8, LANES), f32),
        pltpu.VMEM((256, 256), bf16),
        pltpu.VMEM((slots, LANES), bf16),
        pltpu.VMEM((2 * pad_rows, slots), bf16),
        pltpu.VMEM((LANES, LANES), f32),
        pltpu.VMEM((n_tp, pad_rows, LANES), bf16),
        pltpu.VMEM((n_ep, 2, LANES), bf16),
        pltpu.VMEM((n_ep + ALONE, 2, LANES), bf16),
        pltpu.VMEM((n_tp, slots + 2 * ALONE, LANES), bf16),
        pltpu.VMEM((n_tp, slots + 2 * ALONE, LANES), bf16),
        pltpu.VMEM((n_tp, slots + 2 * ALONE, LANES), bf16),
        pltpu.VMEM((n_ep + ALONE, 2, LANES), bf16),
        pltpu.VMEM((n_ep, 2, LANES), bf16),
        dma((13,)),
        dma,
        dma,
        dma,
        dma((3,)),
        dma((3,)),
        dma((3,)),
        dma((3,)),
        dma((3,)),
        dma,
        dma,
        pltpu.SemaphoreType.REGULAR((n_ep // CORES,)),
        pltpu.VMEM((n_tp, 2, LANES), bf16),
        pltpu.VMEM((n_tp, n_ep, 2, LANES), bf16),
        dma,
        dma,
    ]
    shapes = (
        (seq_rows, w_out.shape[1]),
        (seq_rows, w_key.shape[1]),
        (seq_rows, w_value.shape[1]),
    )
    results = pl.pallas_call(
        functools.partial(kernel, n_tp, n_ep),
        out_shape=tuple(pltpu.VMEM(shape, bf16) for shape in shapes),
        in_specs=[pl.BlockSpec(memory_space=pltpu.HBM)] * len(operands),
        out_specs=[pl.BlockSpec(memory_space=pltpu.VMEM)] * 3,
        scratch_shapes=scratch,
        compiler_params=pltpu.CompilerParams(collective_id=0, has_side_effects=True),
    )(*operands)
    return pl.pallas_call(
        write_out,
        out_shape=tuple(jax.ShapeDtypeStruct(shape, bf16) for shape in shapes),
        in_specs=[pl.BlockSpec(memory_space=pltpu.VMEM)] * 3,
        out_specs=[pl.BlockSpec(memory_space=pltpu.HBM)] * 3,
        scratch_shapes=[dma((3,))],
    )(*[pltpu.with_memory_space_constraint(r, pltpu.VMEM) for r in results])


def solution(mesh):
    in_specs = (
        P(("grp", "ep"), None),
        P(),
        P(None, "tp"),
        P(None, "tp"),
        P(None, "tp"),
        P(("grp", "ep"), "tp", None),
        P(("grp", "ep"), "tp", None),
        P(("grp", "ep")),
        P("tp"),
        P(None, "tp"),
        P(),
        P(("grp", "ep"), None),
        P(("grp", "ep"), None),
        P("ep", None, "tp"),
        P("ep", None, "tp"),
        P("ep", "tp", None),
    )
    out_specs = (P(("grp", "ep"), "tp"), P(("grp", "ep"), "tp"), P(("grp", "ep"), "tp"))
    body = functools.partial(shards, mesh.shape["tp"], mesh.shape["ep"])
    return jax.shard_map(body, mesh=mesh, in_specs=in_specs, out_specs=out_specs, check_vma=False)
```

```python
import functools

import jax
import jax.numpy as jnp
from jax import lax
from jax.experimental import pallas as pl
from jax.experimental.pallas import tpu as pltpu
from jax.sharding import PartitionSpec as P

HEAD_SIZE = 64
LANES = 128
CORES = 2
ALONE = 8
epsilon = 1e-06
f32 = jnp.float32
bf16 = jnp.bfloat16


def iota(shape, dim):
    return lax.broadcasted_iota(jnp.int32, shape, dim)


def hops(step, count):
    return min(step % count, -step % count)


def far_first(count):
    return sorted(range(1, count), key=lambda step: -hops(step, count))


def near_first(count):
    return sorted(range(1, count), key=lambda step: hops(step, count))


def nt_dot(left, right):
    return lax.dot_general(left, right, (((1,), (1,)), ((), ())), preferred_element_type=f32)


def kernel(
    n_tp,
    n_ep,
    tok_hbm,
    again_hbm,
    wq_hbm,
    wk_hbm,
    wv_hbm,
    key_hbm,
    val_hbm,
    len_hbm,
    bias_hbm,
    wo_hbm,
    fgain_hbm,
    ids_hbm,
    rw_hbm,
    wg_hbm,
    wu_hbm,
    wd_hbm,
    mixed_ref,
    nk_ref,
    nv_ref,
    tok,
    again,
    wq,
    wk,
    wv,
    key,
    val,
    lens,
    bias,
    wo,
    fgain,
    ids,
    rw,
    wg,
    wu,
    wd,
    rows_pad,
    idp,
    rwp,
    tri,
    place,
    combine,
    hid,
    hg,
    zsend,
    zrecv,
    xg,
    rsend,
    rrecv,
    ysend,
    ret,
    local_sem,
    h_ssem,
    h_rsem,
    z_ssem,
    z_rsem,
    g_ssem,
    g_rsem,
    r_ssem,
    r_rsem,
    y_ssem,
    y_rsem,
    ready,
    psend,
    terms,
    p_ssem,
    p_rsem,
):
    tp = lax.axis_index("tp")
    ep = lax.axis_index("ep")
    core = lax.rem(ep, CORES)
    chip = ep // CORES
    chips = n_ep // CORES
    seq_rows = tok.shape[0]
    slots = 2 * n_ep

    def copies_of(first, pairs):
        made = [
            pltpu.make_async_copy(source, target, local_sem.at[first + number])
            for number, (source, target) in enumerate(pairs)
        ]
        for copy in made:
            copy.start()
        return made

    c_tok, c_again, c_wq, c_len, c_bias, c_key, c_val = copies_of(
        0,
        (
            (tok_hbm, tok),
            (again_hbm, again),
            (wq_hbm, wq),
            (len_hbm, lens),
            (bias_hbm, bias),
            (key_hbm, key),
            (val_hbm, val),
        ),
    )

    def wrap(number, count):
        return jnp.where(number >= count, number - count, number)

    barrier = pltpu.get_barrier_semaphore()
    column = tp == 0
    topmost = jnp.logical_and(column, ep == 0)
    partner = chip * CORES + (1 - core)
    for step in far_first(n_tp):
        pl.semaphore_signal(barrier, inc=1, device_id={"tp": wrap(tp + step, n_tp)})

    @pl.loop(jnp.where(topmost, n_ep, ep + 1), n_ep)
    def _(above):
        pl.semaphore_signal(barrier, inc=1, device_id={"ep": above})

    @pl.when(jnp.logical_and(column, ep > 0))
    def _():
        pl.semaphore_signal(barrier, inc=1, device_id={"ep": 0})

    def landed(view, sem):
        pltpu.make_async_copy(view, view, sem).wait()

    tri_len = tri.shape[0]
    tri[...] = (iota((tri_len, tri_len), 0) > iota((tri_len, tri_len), 1)).astype(f32).astype(bf16)
    rows_pad[...] = jnp.zeros_like(rows_pad)
    hid[...] = jnp.zeros_like(hid)
    zrecv[pl.ds(1, ALONE - 1)] = jnp.zeros((ALONE - 1, 2, LANES), bf16)
    zrecv[ALONE + n_ep // 4 - 1] = jnp.zeros((2, LANES), bf16)
    idp[...] = jnp.full(idp.shape, -1.0, f32)
    rwp[...] = jnp.zeros_like(rwp)

    c_tok.wait()
    c_again.wait()
    token_rows = tok[...].astype(f32)
    mean_sq = jnp.mean(token_rows * token_rows, axis=1, keepdims=True)
    normed = (token_rows * lax.rsqrt(mean_sq + epsilon) * again[...]).astype(bf16)
    c_wq.wait()
    queries = jnp.dot(normed, wq[...], preferred_element_type=f32).astype(bf16).astype(f32)
    rows_pad[pl.ds(0, seq_rows), :] = queries * HEAD_SIZE ** (-0.5)
    padded = rows_pad[...]
    pad_rows = padded.shape[0]
    low = iota(padded.shape, 1) < HEAD_SIZE
    turned = pltpu.roll(padded, HEAD_SIZE, axis=1)
    both = jnp.concatenate([jnp.where(low, padded, turned), jnp.where(low, turned, padded)], axis=0)
    cols = key.shape[0]
    wide = jnp.concatenate([both] * (cols // LANES), axis=1)
    own_block = (iota(wide.shape, 1) // HEAD_SIZE) == lax.rem(iota(wide.shape, 0), pad_rows)
    spread = jnp.where(own_block, wide, 0.0).astype(bf16)

    c_len.wait()
    c_bias.wait()
    idp[pl.ds(2, 1), pl.ds(0, seq_rows)] = lens[...].astype(f32)
    len_row = jnp.broadcast_to(idp[pl.ds(2, 1), :], (2 * pad_rows, LANES))
    own_lane = iota(len_row.shape, 1) == lax.rem(iota(len_row.shape, 0), pad_rows)
    len_col = jnp.sum(jnp.where(own_lane, len_row, 0.0), axis=1, keepdims=True)
    bias_col = jnp.where(
        iota((2 * pad_rows, 1), 0) < pad_rows, bias[pl.ds(0, 1), pl.ds(0, 1)], bias[pl.ds(0, 1), pl.ds(1, 1)]
    )

    c_key.wait()
    c_wo, c_wk, c_wv, c_ids, c_rw, c_fgain = copies_of(
        7, ((wo_hbm, wo), (wk_hbm, wk), (wv_hbm, wv), (ids_hbm, ids), (rw_hbm, rw), (fgain_hbm, fgain))
    )
    scores = jnp.dot(spread, key[...], preferred_element_type=f32) + bias_col
    in_cache = iota(scores.shape, 1).astype(f32) < len_col
    log_rest = -(jnp.maximum(scores, 0.0) + jnp.log1p(jnp.exp(-jnp.abs(scores))))
    log_rest = jnp.where(in_cache, log_rest, 0.0)
    cache_len = scores.shape[1]
    chunk_count = cache_len // tri_len
    high = log_rest.astype(bf16)
    rest = (log_rest - high.astype(f32)).astype(bf16)
    stacked = jnp.concatenate(
        [part[:, c * tri_len : (c + 1) * tri_len] for part in (high, rest) for c in range(chunk_count)], axis=0
    )
    within = jnp.dot(stacked, tri[...], preferred_element_type=f32)
    tails = []
    carry = jnp.zeros((2 * pad_rows, 1), f32)
    span = 2 * pad_rows
    for c in reversed(range(chunk_count)):
        inner = within[c * span : (c + 1) * span] + within[(chunk_count + c) * span : (chunk_count + c + 1) * span]
        tails.append(inner + carry)
        carry = carry + inner[:, 0:1] + log_rest[:, c * tri_len : c * tri_len + 1]
    tail = jnp.concatenate(tails[::-1], axis=1)
    breaks = jnp.where(in_cache, jnp.exp(scores + log_rest + tail), 0.0).astype(bf16)
    c_val.wait()
    mixed_values = nt_dot(breaks, val[...])
    mixed_values = jnp.where(own_block, mixed_values, 0.0)
    folded = mixed_values[:, 0:LANES]
    for c in range(1, cols // LANES):
        folded = folded + mixed_values[:, c * LANES : (c + 1) * LANES]
    folded = folded + pltpu.roll(folded, HEAD_SIZE, axis=1)
    heads = jnp.where(low, folded[:pad_rows], folded[pad_rows:]).astype(bf16)
    hg[tp] = heads

    lowest = jnp.where(column, 1, 0)
    pl.semaphore_wait(barrier, (n_tp - 1) + jnp.where(topmost, n_ep - 1, ep - lowest))
    for step in far_first(n_tp):
        pltpu.make_async_remote_copy(
            hg.at[tp], hg.at[tp], h_ssem, h_rsem, device_id={"tp": wrap(tp + step, n_tp)}
        ).start()

    @pl.loop(lowest, jnp.where(topmost, n_ep, ep))
    def _(below):
        pl.semaphore_signal(ready.at[chip], inc=1, device_id={"ep": below})

    c_wg, c_wu, c_wd = copies_of(0, ((wg_hbm, wg), (wu_hbm, wu), (wd_hbm, wd)))
    c_wk.wait()
    c_wv.wait()
    nk_ref[...] = nt_dot(normed, wk[...]).astype(bf16)
    nv_ref[...] = nt_dot(normed, wv[...]).astype(bf16)
    c_ids.wait()
    c_rw.wait()
    top_count = ids.shape[0]
    idp[pl.ds(0, top_count), pl.ds(0, seq_rows)] = ids[...].astype(f32)
    rwp[pl.ds(0, top_count), pl.ds(0, seq_rows)] = rw[...]
    slot_expert = (iota((slots, LANES), 0) // 2).astype(f32)
    slot_rank = lax.rem(iota((slots, LANES), 0), 2).astype(f32)
    hits = [(slot_expert == idp[pl.ds(k, 1), :]).astype(f32) for k in range(top_count)]
    any_hit = sum(hits)
    upper = (iota((LANES, LANES), 0) < iota((LANES, LANES), 1)).astype(f32).astype(bf16)
    before = jnp.dot(any_hit.astype(bf16), upper, preferred_element_type=f32)
    taken = jnp.where(before == slot_rank, 1.0, 0.0)
    place[...] = (any_hit * taken).astype(bf16)
    weighted = sum(hits[k] * rwp[pl.ds(k, 1), :] for k in range(top_count)) * taken
    weighted_t = weighted.T[: combine.shape[0] // 2]
    weighted_high = weighted_t.astype(bf16)
    combine[pl.ds(0, pad_rows), :] = weighted_high
    combine[pl.ds(pad_rows, pad_rows), :] = (weighted_t - weighted_high.astype(f32)).astype(bf16)
    c_fgain.wait()
    own_cols = pl.ds(pl.multiple_of(tp * LANES, LANES), LANES)
    own_tokens = tok[:, own_cols].astype(f32)
    own_gain = fgain[:, own_cols]

    c_wo.wait()
    inverse_sq = 1.0 / (fgain[...] * fgain[...])
    peers = pl.ds(0, n_tp - 1)
    landed(hg.at[peers], h_rsem)
    all_heads = jnp.concatenate([hg[peer] for peer in range(n_tp)], axis=1)
    attn_out = jnp.dot(all_heads, wo[...], preferred_element_type=f32)
    hid[pl.ds(0, seq_rows), :] = own_tokens + attn_out[:seq_rows]
    scaled = (hid[...] * own_gain).astype(bf16)
    outgoing = jnp.dot(place[...], scaled, preferred_element_type=f32).astype(bf16)
    zsend[...] = outgoing.reshape(zsend.shape)

    quarter = n_ep // 4
    groups = ((0, 1, 0, ALONE), (1, quarter, ALONE, quarter), (quarter, n_ep, ALONE + quarter, n_ep - quarter))
    own_group = jnp.where(ep == 0, 0, jnp.where(ep < quarter, 1, 2))
    own_entry = jnp.where(ep == 0, 0, jnp.where(ep < quarter, ep + (ALONE - 1), ep + ALONE))
    def send_slots(to_ep):
        @pl.when(to_ep != ep)
        def _():
            pltpu.make_async_remote_copy(
                zsend.at[to_ep], zrecv.at[own_entry], z_ssem, z_rsem.at[own_group], device_id={"ep": to_ep}
            ).start()

    @pl.when(jnp.logical_not(column))
    def _():
        send_slots(0)

    for turn, far_chip in enumerate(far_first(chips) + [0]):
        to_chip = jnp.where(ep == 0, far_chip, turn)
        if turn == chips - 1:

            @pl.when(jnp.logical_and(column, ep > 0))
            def _():
                pl.semaphore_wait(ready.at[0], 1)
                send_slots(0)

        @pl.when(jnp.logical_and(to_chip > chip, jnp.logical_not(topmost)))
        def _():
            pl.semaphore_wait(ready.at[to_chip], CORES)

        @pl.when(jnp.logical_and(jnp.logical_and(to_chip == chip, core == 0), jnp.logical_not(topmost)))
        def _():
            pl.semaphore_wait(ready.at[to_chip], 1)

        for to_core in range(CORES):
            to_ep = to_chip * CORES + to_core

            @pl.when(to_ep > 0)
            def _():
                send_slots(to_ep)

    pltpu.make_async_copy(zsend.at[ep], zrecv.at[own_entry], z_rsem.at[own_group]).start()

    c_wg.wait()
    c_wu.wait()
    c_wd.wait()
    def gather(group):
        first, last, entry, width = groups[group]
        here = pl.ds(2 * entry, 2 * width)
        landed(zrecv.at[pl.ds(entry, last - first)], z_rsem.at[group])
        xg[tp, here] = zrecv[pl.ds(entry, width)].reshape(2 * width, LANES)
        for step in far_first(n_tp):
            pltpu.make_async_remote_copy(
                xg.at[tp, here],
                xg.at[tp, here],
                g_ssem.at[group],
                g_rsem.at[group],
                device_id={"tp": wrap(tp + step, n_tp)},
            ).start()

    def experts(group):
        here = pl.ds(2 * groups[group][2], 2 * groups[group][3])
        landed(xg.at[peers, here], g_rsem.at[group])
        rows = jnp.concatenate([xg[peer, here] for peer in range(n_tp)], axis=1)
        gate = jnp.dot(rows, wg[...], preferred_element_type=f32)
        up = jnp.dot(rows, wu[...], preferred_element_type=f32)
        plain = rows.astype(f32)
        sum_sq = jnp.sum(plain * plain * inverse_sq, axis=1, keepdims=True)
        scale = lax.rsqrt(sum_sq / (n_tp * LANES) + epsilon)
        gate = gate * scale
        up = up * scale
        hidden_act = (gate / (1.0 + jnp.exp(-gate)) * up).astype(bf16)
        partial_value = jnp.dot(hidden_act, wd[...], preferred_element_type=f32).astype(bf16)
        if group == 0:
            for c in range(n_tp):
                psend[c] = partial_value[:2, c * LANES : (c + 1) * LANES]
            for step in far_first(n_tp):
                peer = wrap(tp + step, n_tp)
                pltpu.make_async_remote_copy(
                    psend.at[peer], terms.at[tp, ep], p_ssem, p_rsem, device_id={"ep": 0, "tp": peer}
                ).start()

            @pl.when(ep > 0)
            def _():
                pltpu.make_async_remote_copy(
                    psend.at[tp], terms.at[tp, ep], p_ssem, p_rsem, device_id={"ep": 0}
                ).start()

            @pl.when(ep == 0)
            def _():
                pltpu.make_async_copy(psend.at[tp], terms.at[tp, ep], p_rsem).start()

            return
        for c in range(n_tp):
            rsend[c, here] = partial_value[:, c * LANES : (c + 1) * LANES]
        for step in far_first(n_tp):
            peer = wrap(tp + step, n_tp)
            pltpu.make_async_remote_copy(
                rsend.at[peer, here], rrecv.at[tp, here], r_ssem.at[group], r_rsem.at[group], device_id={"tp": peer}
            ).start()
        rrecv[tp, here] = rsend[tp, here]

    def give_back(group):
        first, last, entry, width = groups[group]
        here = pl.ds(2 * entry, 2 * width)
        landed(rrecv.at[peers, here], r_rsem.at[group])
        total = rrecv[0, here].astype(f32)
        for peer in range(1, n_tp):
            total += rrecv[peer, here].astype(f32)
        ysend[pl.ds(entry, width)] = total.astype(bf16).reshape(width, 2, LANES)
        for to_ep in range(first, last):

            @pl.when(to_ep != ep)
            def _():
                pltpu.make_async_remote_copy(
                    ysend.at[entry + to_ep - first], ret.at[ep], y_ssem, y_rsem, device_id={"ep": to_ep}
                ).start()

    gather(1)
    gather(0)
    experts(1)
    experts(0)
    gather(2)
    give_back(1)
    experts(2)
    give_back(2)
    @pl.when(ep > 0)
    def _():
        pltpu.make_async_copy(ysend.at[own_entry], ret.at[ep], y_rsem).start()
        landed(ret, y_rsem)

    @pl.when(ep == 0)
    def _():
        landed(terms, p_rsem)
        total = terms[0].astype(f32)
        for peer in range(1, n_tp):
            total += terms[peer].astype(f32)
        ret[...] = total.astype(bf16)

    picked = jnp.dot(combine[...], ret[...].reshape(slots, LANES), preferred_element_type=f32)
    routed_sum = picked[:pad_rows] + picked[pad_rows:]
    mixed_ref[...] = (hid[pl.ds(0, seq_rows), :] + routed_sum[:seq_rows]).astype(bf16)
    landed(hg.at[peers], h_ssem)
    landed(zsend.at[pl.ds(0, n_ep - 1)], z_ssem)
    for group, (_, _, entry, width) in enumerate(groups):
        here = pl.ds(2 * entry, 2 * width)
        landed(xg.at[peers, here], g_ssem.at[group])
        if group:
            landed(rsend.at[peers, here], r_ssem.at[group])

    @pl.when(ep > 0)
    def _():
        landed(psend, p_ssem)
        landed(ysend.at[pl.ds(0, n_ep - 2)], y_ssem)

    @pl.when(ep == 0)
    def _():
        landed(psend.at[peers], p_ssem)
        landed(ysend.at[pl.ds(0, n_ep - 1)], y_ssem)


def write_out(*refs):
    count = len(refs) // 2
    copies = [pltpu.make_async_copy(refs[n], refs[count + n], refs[-1].at[n]) for n in range(count)]
    for copy in copies:
        copy.start()
    for copy in copies:
        copy.wait()


def shards(
    n_tp,
    n_ep,
    tokens,
    attn_gain,
    w_query,
    w_key,
    w_value,
    key_cache,
    value_cache,
    lengths,
    head_bias,
    w_out,
    ffn_gain,
    route_ids,
    route_weights,
    w_gate,
    w_up,
    w_down,
):
    seq_rows, model_width = tokens.shape
    cache_len = key_cache.shape[2]
    kv_cols = key_cache.shape[1]
    pad_rows = 16
    slots = 2 * n_ep
    operands = (
        tokens,
        attn_gain.reshape(1, model_width),
        w_query,
        w_key.T,
        w_value.T,
        key_cache.reshape(seq_rows * kv_cols, cache_len),
        value_cache.reshape(seq_rows * kv_cols, cache_len),
        lengths.reshape(1, seq_rows),
        head_bias.reshape(1, head_bias.shape[0]),
        w_out,
        ffn_gain.reshape(1, model_width),
        route_ids.T,
        route_weights.T,
        w_gate[0],
        w_up[0],
        w_down[0],
    )
    dma = pltpu.SemaphoreType.DMA
    scratch = [pltpu.VMEM(op.shape, op.dtype) for op in operands] + [
        pltpu.VMEM((pad_rows, LANES), f32),
        pltpu.VMEM((8, LANES), f32),
        pltpu.VMEM((8, LANES), f32),
        pltpu.VMEM((256, 256), bf16),
        pltpu.VMEM((slots, LANES), bf16),
        pltpu.VMEM((2 * pad_rows, slots), bf16),
        pltpu.VMEM((LANES, LANES), f32),
        pltpu.VMEM((n_tp, pad_rows, LANES), bf16),
        pltpu.VMEM((n_ep, 2, LANES), bf16),
        pltpu.VMEM((n_ep + ALONE, 2, LANES), bf16),
        pltpu.VMEM((n_tp, slots + 2 * ALONE, LANES), bf16),
        pltpu.VMEM((n_tp, slots + 2 * ALONE, LANES), bf16),
        pltpu.VMEM((n_tp, slots + 2 * ALONE, LANES), bf16),
        pltpu.VMEM((n_ep + ALONE, 2, LANES), bf16),
        pltpu.VMEM((n_ep, 2, LANES), bf16),
        dma((13,)),
        dma,
        dma,
        dma,
        dma((3,)),
        dma((3,)),
        dma((3,)),
        dma((3,)),
        dma((3,)),
        dma,
        dma,
        pltpu.SemaphoreType.REGULAR((n_ep // CORES,)),
        pltpu.VMEM((n_tp, 2, LANES), bf16),
        pltpu.VMEM((n_tp, n_ep, 2, LANES), bf16),
        dma,
        dma,
    ]
    shapes = (
        (seq_rows, w_out.shape[1]),
        (seq_rows, w_key.shape[1]),
        (seq_rows, w_value.shape[1]),
    )
    results = pl.pallas_call(
        functools.partial(kernel, n_tp, n_ep),
        out_shape=tuple(pltpu.VMEM(shape, bf16) for shape in shapes),
        in_specs=[pl.BlockSpec(memory_space=pltpu.HBM)] * len(operands),
        out_specs=[pl.BlockSpec(memory_space=pltpu.VMEM)] * 3,
        scratch_shapes=scratch,
        compiler_params=pltpu.CompilerParams(collective_id=0, has_side_effects=True),
    )(*operands)
    return pl.pallas_call(
        write_out,
        out_shape=tuple(jax.ShapeDtypeStruct(shape, bf16) for shape in shapes),
        in_specs=[pl.BlockSpec(memory_space=pltpu.VMEM)] * 3,
        out_specs=[pl.BlockSpec(memory_space=pltpu.HBM)] * 3,
        scratch_shapes=[dma((3,))],
    )(*[pltpu.with_memory_space_constraint(r, pltpu.VMEM) for r in results])


def solution(mesh):
    in_specs = (
        P(("grp", "ep"), None),
        P(),
        P(None, "tp"),
        P(None, "tp"),
        P(None, "tp"),
        P(("grp", "ep"), "tp", None),
        P(("grp", "ep"), "tp", None),
        P(("grp", "ep")),
        P("tp"),
        P(None, "tp"),
        P(),
        P(("grp", "ep"), None),
        P(("grp", "ep"), None),
        P("ep", None, "tp"),
        P("ep", None, "tp"),
        P("ep", "tp", None),
    )
    out_specs = (P(("grp", "ep"), "tp"), P(("grp", "ep"), "tp"), P(("grp", "ep"), "tp"))
    body = functools.partial(shards, mesh.shape["tp"], mesh.shape["ep"])
    return jax.shard_map(body, mesh=mesh, in_specs=in_specs, out_specs=out_specs, check_vma=False)
```
